32 devices in a mesh: grp: 2 (over x), st: 4 (over y, core), tp: 4 (over z).
Axes of the slice: x: 2, y: 2, z: 4, core: 2. Of those that a mesh axis runs over, the one named last changes fastest.
Arguments:
- tokens: bfloat16 [4096, 2048], P(('grp', 'st')), parts along dimension 0, may hold values from -6 to 6, as said below
- store: bfloat16 [64, 128, 2048], P(('grp', 'st')), parts along dimension 0, may hold values from -6 to 6, as said below
- passage_ids: int32 [64, 4], P(('grp', 'st')), parts along dimension 0, may hold values from 0 to 31, as said below
- mix_gain: float32 [2048], replicated, may hold values from 0.1 to 1.9
- glu_value: bfloat16 [2048, 1024], P(None, 'tp'), may hold values from -0.125 to 0.125
- glu_gate: bfloat16 [2048, 1024], P(None, 'tp'), may hold values from -0.125 to 0.125
- conv_taps: bfloat16 [31, 1024], P(None, 'tp'), may hold values from -5 to 5
- channel_gain: float32 [1024], P('tp'), may hold values from 0.1 to 1.9
- mix_out: bfloat16 [1024, 2048], P('tp'), may hold values from -0.1875 to 0.1875
- query_gain: float32 [2048], replicated, may hold values from 0.1 to 1.9
- passage_gain: float32 [2048], replicated, may hold values from 0.1 to 1.9
- query_proj: bfloat16 [2048, 2048], P(None, 'tp'), may hold values from -1 to 1
- key_proj: bfloat16 [2048, 2048], P(None, 'tp'), may hold values from -1 to 1
- value_proj: bfloat16 [2048, 2048], P(None, 'tp'), may hold values from -0.125 to 0.125
- attn_out: bfloat16 [2048, 2048], P('tp'), may hold values from -0.125 to 0.125
- blend_gain: float32 [2048], replicated, may hold values from 0.5 to 3
Outputs:
- blended: bfloat16 [4096, 2048], P(('grp', 'st', 'tp')), parts along dimension 0
The draws below stay inside these ranges and needn't reach their ends.
There are 2 independent parts, one for each index of `grp`. The reference program is written for one: setup_inputs(seed, part) draws one part's arguments, and reference() takes and returns one part's arrays. A program takes and returns all parts, laid end to end along the dimension named above; an argument that names none is the same for every part. Nothing has to cross between parts.
Inputs may be any that keep to these rules, and one draw needn't show every extreme that they name: `tokens`: standard normal entries clipped to the range. `store`: standard normal entries clipped to the range. `passage_ids`: passage p is held by index p // 8 of st. The 32 requests of the 8 blocks of one index of st (repeats counted) name at most 16 passages held by any one index of st, and in every draw one index of st receives exactly 16 requests from every index of st.
All inputs are finite; a program needn't handle non-finite values.
Results may differ from the reference program's by a relative error of at most 0.01575.
The reference program's roundings to bfloat16 on the way count: a program that leaves them out, or rounds other values in their place, can miss the bound.
Values may be sent and summed in bfloat16 or wider, within the bound.
A program may use at most 128 MiB of HBM per device.

```python
import jax
import jax.numpy as jnp
from jax import lax

D = 2048
CA = 1024
HEADS = 8
KW = 31
SEQ_LEN = 128
BLK = 64
NP = 4
PROWS = 128
PASS_DEV = 8
TOKENS = 2048
NB_DEV = 8
BLOCKS = 32
RQ = 32
MOST = 16
PASSAGES = 32
N_ST = 4
N_TP = 4


def request_table(key):
    hot_owner = jax.random.randint(jax.random.fold_in(key, 1), (), 0, N_ST)
    positions = jnp.arange(RQ)

    def one_device(device, dev_key):
        first_turn = (device - 1 - hot_owner) % N_ST - 1
        spread_turn = (first_turn + positions - MOST) % (N_ST - 1)
        owners_of = jnp.where(positions < MOST, hot_owner, (hot_owner + 1 + spread_turn) % N_ST)
        owners_of = owners_of[jax.random.permutation(dev_key, RQ)]
        local_index = jax.random.randint(jax.random.fold_in(dev_key, 3), (RQ,), 0, PASS_DEV)
        return (owners_of * PASS_DEV + local_index).reshape(NB_DEV, NP)
    dev_keys = jax.random.split(jax.random.fold_in(key, 2), N_ST)
    table = jax.vmap(one_device)(jnp.arange(N_ST), dev_keys)
    return table.reshape(BLOCKS, NP).astype(jnp.int32)


def store_rows(key):
    return jnp.clip(jax.random.normal(jax.random.fold_in(key, 12), (PASSAGES, PROWS, D), jnp.float32), -6.0, 6.0)


def draw_passage_ids(key, part):
    return request_table(jax.random.fold_in(key, 11))


def draw_store(key, part):
    return store_rows(key).astype(jnp.bfloat16)


def draw_tokens(key, part):
    plain_rows = jnp.clip(jax.random.normal(jax.random.fold_in(key, 13), (TOKENS, D), jnp.float32), -6.0, 6.0)
    return plain_rows.astype(jnp.bfloat16)


def draw_conv_taps(key, part):
    channel = jnp.arange(CA).astype(jnp.float32)
    channel_scale = jnp.exp(1.5 * (2.0 * channel / CA - 1.0)) * KW ** (-0.5)
    tap_draw = jnp.clip(jax.random.normal(jax.random.fold_in(key, 31), (KW, CA), jnp.float32), -6.0, 6.0)
    return jnp.clip(tap_draw * channel_scale, -5.0, 5.0).astype(jnp.bfloat16)


def draw_query_proj(key, part):
    fresh_draw = jax.random.normal(jax.random.fold_in(key, 22), (D, D), jnp.float32) * D ** (-0.5)
    return jnp.clip(fresh_draw, -1.0, 1.0).astype(jnp.bfloat16)


def draw_key_proj(key, part):
    fresh_draw = jax.random.normal(jax.random.fold_in(key, 23), (D, D), jnp.float32) * D ** (-0.5)
    return jnp.clip(fresh_draw, -1.0, 1.0).astype(jnp.bfloat16)


def shard_levels(stream_key, dims, pieces, smallest, high):
    gain, own = 1.0, jax.random.fold_in(stream_key, 6)
    for axis_at, blocks in pieces:
        steps = jnp.exp(jax.random.uniform(jax.random.fold_in(own, axis_at), (blocks,), jnp.float32, smallest / len(pieces), high / len(pieces)))
        gain = gain * jnp.repeat(steps, dims[axis_at] // blocks).reshape([-1 if axis == axis_at else 1 for axis in range(len(dims))])
    return gain


def normal_values(own_key, dims, scale, reach, cuts=(), dtype=jnp.bfloat16):
    drawn = jax.random.normal(own_key, dims, jnp.float32) * scale
    if len(cuts) > 0:
        drawn = shard_levels(own_key, dims, cuts, -0.22, 0.18) * drawn
    return jnp.clip(drawn, min=-reach, max=reach).astype(dtype)


def setup_inputs(seed: int = 0, part: int = 0) -> dict:
    streams_of = jax.random.split(jax.random.key(seed), 17)
    part_keys = jax.random.split(jax.random.fold_in(streams_of[16], part), 17)
    return {
        "tokens": draw_tokens(jax.random.fold_in(jax.random.fold_in(streams_of[16], part), 71), part),
        "store": draw_store(jax.random.fold_in(jax.random.fold_in(streams_of[16], part), 71), part),
        "passage_ids": draw_passage_ids(jax.random.fold_in(jax.random.fold_in(streams_of[16], part), 71), part),
        "mix_gain": jnp.clip(1.0 + 0.18 * jax.random.normal(streams_of[3], (D,), jnp.float32), 0.1, 1.9),
        "glu_value": normal_values(streams_of[4], (D, CA), D ** -0.5, 0.125, ((1, 4),)),
        "glu_gate": normal_values(streams_of[5], (D, CA), D ** -0.5, 0.125, ((1, 4),)),
        "conv_taps": draw_conv_taps(jax.random.fold_in(streams_of[16], 71), part),
        "channel_gain": jnp.clip(1.0 + 0.18 * jax.random.normal(streams_of[7], (CA,), jnp.float32), 0.1, 1.9),
        "mix_out": normal_values(streams_of[8], (CA, D), CA ** -0.5, 0.1875, ((0, 4),)),
        "query_gain": jnp.clip(1.0 + 0.18 * jax.random.normal(streams_of[9], (D,), jnp.float32), 0.1, 1.9),
        "passage_gain": jnp.clip(1.0 + 0.18 * jax.random.normal(streams_of[10], (D,), jnp.float32), 0.1, 1.9),
        "query_proj": draw_query_proj(jax.random.fold_in(streams_of[16], 71), part),
        "key_proj": draw_key_proj(jax.random.fold_in(streams_of[16], 71), part),
        "value_proj": normal_values(streams_of[13], (D, D), D ** -0.5, 0.125, ((1, 4),)),
        "attn_out": normal_values(streams_of[14], (D, D), D ** -0.5, 0.125, ((0, 4),)),
        "blend_gain": jnp.clip(jax.random.uniform(streams_of[15], (D,), jnp.float32, 0.5, 3.0), 0.5, 3.0),
    }


EPS = 1e-06

def rms_rows(row_data, gain_vec):
    floats = row_data.astype(jnp.float32)
    inv_scale = lax.rsqrt(lax.optimization_barrier(jnp.mean(floats * floats, axis=-1, keepdims=True)) + EPS)
    return (floats * inv_scale * gain_vec.astype(jnp.float32)).astype(jnp.bfloat16)

def depthwise(gated_rows, conv_taps):
    span_width = conv_taps.shape[0]
    half_span = (span_width - 1) // 2
    seq_length = gated_rows.shape[1]
    padded = jnp.pad(gated_rows.astype(jnp.float32), ((0, 0), (half_span, span_width - 1 - half_span), (0, 0)))
    running = jnp.zeros(gated_rows.shape, jnp.float32)
    for tap_index in range(span_width):
        running = running + padded[:, tap_index:tap_index + seq_length] * conv_taps[tap_index].astype(jnp.float32)
    return running

def passage_attention(queries, keys_values, head_count):
    groups, block_len, span_width = queries.shape
    head_dim = span_width // head_count
    row_count = keys_values.shape[1]
    query_heads = queries.astype(jnp.float32).reshape(groups, block_len, head_count, head_dim)
    key_heads = keys_values[:, :, :span_width].astype(jnp.float32).reshape(groups, row_count, head_count, head_dim)
    value_heads = keys_values[:, :, span_width:].astype(jnp.float32).reshape(groups, row_count, head_count, head_dim)
    scores = jnp.einsum('gqhd,grhd->ghqr', query_heads, key_heads) * head_dim ** (-0.5)
    row_top = lax.optimization_barrier(jnp.max(scores, axis=-1))
    exponent = jnp.exp(scores - row_top[..., None])
    row_sum = lax.optimization_barrier(jnp.sum(exponent, axis=-1))
    weights = exponent.astype(jnp.bfloat16).astype(jnp.float32)
    outputs = jnp.einsum('ghqr,grhd->gqhd', weights, value_heads).astype(jnp.bfloat16)
    return (outputs.reshape(groups, block_len, span_width), row_top, row_sum)

def combine(outs, tops, sums, head_count):
    batch_count, passage_count, block_len, span_width = outs.shape
    head_dim = span_width // head_count
    best_top = lax.optimization_barrier(jnp.max(tops, axis=1, keepdims=True))
    weight = jnp.exp(tops - best_top)
    numerator = jnp.einsum('bphq,bpqhd->bqhd', weight, outs.astype(jnp.float32).reshape(batch_count, passage_count, block_len, head_count, head_dim))
    denominator = lax.optimization_barrier(jnp.sum(weight * sums, axis=1))
    result = numerator / jnp.transpose(denominator, (0, 2, 1))[..., None]
    return result.reshape(batch_count, block_len, span_width).astype(jnp.bfloat16)

def reference(tokens, store, passage_ids, mix_gain, glu_value, glu_gate, conv_taps, channel_gain, mix_out, query_gain, passage_gain, query_proj, key_proj, value_proj, attn_out, blend_gain):
    mix_input = rms_rows(tokens, mix_gain)
    value_part = jnp.dot(mix_input, glu_value, preferred_element_type=jnp.float32)
    gate_part = jnp.dot(mix_input, glu_gate, preferred_element_type=jnp.float32)
    gated_rows = (value_part * jax.nn.sigmoid(gate_part)).astype(jnp.bfloat16)
    conv_rows = depthwise(gated_rows.reshape(-1, SEQ_LEN, CA), conv_taps).reshape(-1, CA)
    row_mean = lax.optimization_barrier(jnp.mean(conv_rows, axis=1, keepdims=True))
    row_var = lax.optimization_barrier(jnp.mean(conv_rows * conv_rows, axis=1, keepdims=True)) - row_mean * row_mean
    activation = jax.nn.silu((conv_rows - row_mean) * lax.rsqrt(row_var + EPS) * channel_gain.astype(jnp.float32)).astype(jnp.bfloat16)
    queries = jnp.dot(rms_rows(tokens, query_gain), query_proj, preferred_element_type=jnp.float32).astype(jnp.bfloat16)
    passage_rows = rms_rows(store.reshape(-1, D), passage_gain)
    key_rows = jnp.dot(passage_rows, key_proj, preferred_element_type=jnp.float32).astype(jnp.bfloat16)
    value_rows = jnp.dot(passage_rows, value_proj, preferred_element_type=jnp.float32).astype(jnp.bfloat16)
    memory = jnp.concatenate([key_rows, value_rows], axis=1).reshape(store.shape[0], store.shape[1], 2 * D)

    def one_block(inputs):
        block_queries, block_ids = inputs
        wanted = memory[block_ids]
        repeated = jnp.broadcast_to(block_queries[None], (NP, BLK, D))
        part_out, part_top, part_sum = passage_attention(repeated, wanted, HEADS)
        return combine(part_out[None], part_top[None], part_sum[None], HEADS)[0]
    attended = lax.map(one_block, (queries.reshape(-1, BLK, D), passage_ids)).reshape(-1, D)
    channel_group = CA // N_TP
    column_group = D // N_TP
    running = jnp.zeros((tokens.shape[0], D), jnp.float32)
    for shard_index in range(N_TP):
        conv_part = jnp.dot(activation[:, shard_index * channel_group:(shard_index + 1) * channel_group], mix_out[shard_index * channel_group:(shard_index + 1) * channel_group], preferred_element_type=jnp.float32)
        attn_part = jnp.dot(attended[:, shard_index * column_group:(shard_index + 1) * column_group], attn_out[shard_index * column_group:(shard_index + 1) * column_group], preferred_element_type=jnp.float32)
        partial_value = (conv_part + blend_gain.astype(jnp.float32) * attn_part).astype(jnp.bfloat16)
        partial_value = lax.optimization_barrier(partial_value)
        running = running + partial_value.astype(jnp.float32)
    return running.astype(jnp.bfloat16)
```

```python
import functools

import jax
import jax.numpy as jnp
from jax import lax
from jax.sharding import PartitionSpec as P
from jax.experimental import pallas as pl
from jax.experimental.pallas import tpu as pltpu

CA = 1024
HD = 256
SEQ_LEN = 128


EPS = 1e-06


def rms_rows(row_data, gain_vec):
    floats = row_data.astype(jnp.float32)
    inv_scale = lax.rsqrt(jnp.mean(floats * floats, axis=-1, keepdims=True) + EPS)
    return (floats * inv_scale * gain_vec).astype(jnp.bfloat16)


def depthwise(gated_rows, conv_taps):
    span_width = conv_taps.shape[0]
    half_span = (span_width - 1) // 2
    seq_length = gated_rows.shape[1]
    padded = jnp.pad(
        gated_rows.astype(jnp.float32), ((0, 0), (half_span, span_width - 1 - half_span), (0, 0))
    )
    running = jnp.zeros(gated_rows.shape, jnp.float32)
    for tap_index in range(span_width):
        running = running + padded[:, tap_index : tap_index + seq_length] * conv_taps[
            tap_index
        ].astype(jnp.float32)
    return running


def passage_attention(queries, keys_values, head_count):
    groups, block_len, span_width = queries.shape
    head_dim = span_width // head_count
    row_count = keys_values.shape[1]
    query_heads = queries.reshape(groups, block_len, head_count, head_dim)
    key_heads = keys_values[:, :, :span_width].reshape(groups, row_count, head_count, head_dim)
    value_heads = keys_values[:, :, span_width:].reshape(groups, row_count, head_count, head_dim)
    scores = jnp.einsum(
        "gqhd,grhd->ghqr", query_heads, key_heads, preferred_element_type=jnp.float32
    ) * head_dim ** (-0.5)
    row_top = jnp.max(scores, axis=-1)
    exponent = jnp.exp(scores - row_top[..., None])
    row_sum = jnp.sum(exponent, axis=-1)
    weights = exponent.astype(jnp.bfloat16)
    outputs = jnp.einsum(
        "ghqr,grhd->gqhd", weights, value_heads, preferred_element_type=jnp.float32
    ).astype(jnp.bfloat16)
    return (outputs.reshape(groups, block_len, span_width), row_top, row_sum)


def combine(outs, tops, sums, head_count):
    batch_count, passage_count, block_len, span_width = outs.shape
    head_dim = span_width // head_count
    best_top = jnp.max(tops, axis=1, keepdims=True)
    weight = jnp.exp(tops - best_top)
    numerator = jnp.einsum(
        "bphq,bpqhd->bqhd",
        weight,
        outs.astype(jnp.float32).reshape(
            batch_count, passage_count, block_len, head_count, head_dim
        ),
    )
    denominator = jnp.sum(weight * sums, axis=1)
    result = numerator / jnp.transpose(denominator, (0, 2, 1))[..., None]
    return result.reshape(batch_count, block_len, span_width).astype(jnp.bfloat16)


def local(
    tokens,
    store,
    passage_ids,
    mix_gain,
    glu_value,
    glu_gate,
    conv_taps,
    channel_gain,
    mix_out,
    query_gain,
    passage_gain,
    query_proj,
    key_proj,
    value_proj,
    attn_out,
    blend_gain,
):
    owners = lax.axis_size("st")
    tok_rows = tokens.shape[0]
    model_width = tokens.shape[1]
    local_channels = glu_value.shape[1]
    head_width = query_proj.shape[1]
    local_heads = head_width // HD
    block_count = passage_ids.shape[0]
    per_block = passage_ids.shape[1]
    block_len = tok_rows // block_count
    requests = block_count * per_block
    capacity = 2 * requests // owners
    pass_local = store.shape[0]
    pass_rows = store.shape[1]
    flat_ids = passage_ids.reshape(requests)
    owner_of = flat_ids // pass_local
    local_of = flat_ids - owner_of * pass_local
    request_index = jnp.arange(requests)
    earlier = (owner_of[:, None] == owner_of[None, :]) & (
        request_index[None, :] < request_index[:, None]
    )
    ranking = jnp.sum(earlier.astype(jnp.int32), axis=1)
    slot_of = owner_of * capacity + ranking
    slot_ids = (
        jnp.zeros((owners * capacity,), jnp.int32)
        .at[slot_of]
        .set(local_of)
        .reshape(owners, capacity)
    )
    asked = lax.all_to_all(slot_ids, "st", split_axis=0, concat_axis=0, tiled=True)
    normed_store = rms_rows(store.reshape(pass_local * pass_rows, model_width), passage_gain)
    key_rows = jnp.dot(normed_store, key_proj, preferred_element_type=jnp.float32).astype(
        jnp.bfloat16
    )
    value_rows = jnp.dot(normed_store, value_proj, preferred_element_type=jnp.float32).astype(
        jnp.bfloat16
    )
    memory = jnp.concatenate([key_rows, value_rows], axis=1).reshape(
        pass_local, pass_rows, 2 * head_width
    )
    queries = jnp.dot(
        rms_rows(tokens, query_gain), query_proj, preferred_element_type=jnp.float32
    ).astype(jnp.bfloat16)
    query_blocks = queries.reshape(block_count, block_len, head_width)
    repeated = jnp.repeat(query_blocks, per_block, axis=0)
    served = memory[asked.reshape(owners * capacity)]
    slot_queries = (
        jnp.zeros((owners * capacity, block_len, head_width), jnp.bfloat16)
        .at[slot_of]
        .set(repeated)
    )
    visiting = lax.all_to_all(
        slot_queries.reshape(owners, capacity, block_len, head_width),
        "st",
        split_axis=0,
        concat_axis=0,
        tiled=True,
    )
    answer_out, answer_top, answer_sum = passage_attention(
        visiting.reshape(owners * capacity, block_len, head_width), served, local_heads
    )
    back_out = lax.all_to_all(
        answer_out.reshape(owners, capacity, block_len, head_width),
        "st",
        split_axis=0,
        concat_axis=0,
        tiled=True,
    )
    back_top, back_sum = (
        lax.all_to_all(
            answer_top.reshape(owners, capacity, local_heads, block_len),
            "st",
            split_axis=0,
            concat_axis=0,
            tiled=True,
        ),
        lax.all_to_all(
            answer_sum.reshape(owners, capacity, local_heads, block_len),
            "st",
            split_axis=0,
            concat_axis=0,
            tiled=True,
        ),
    )
    partial_out = back_out.reshape(owners * capacity, block_len, head_width)[slot_of]
    partial_top = back_top.reshape(owners * capacity, local_heads, block_len)[slot_of]
    partial_sum = back_sum.reshape(owners * capacity, local_heads, block_len)[slot_of]
    attended = combine(
        partial_out.reshape(block_count, per_block, block_len, head_width),
        partial_top.reshape(block_count, per_block, local_heads, block_len),
        partial_sum.reshape(block_count, per_block, local_heads, block_len),
        local_heads,
    ).reshape(tok_rows, head_width)
    mix_input = rms_rows(tokens, mix_gain)
    value_part = jnp.dot(mix_input, glu_value, preferred_element_type=jnp.float32)
    gate_part = jnp.dot(mix_input, glu_gate, preferred_element_type=jnp.float32)
    gated_rows = (value_part * jax.nn.sigmoid(gate_part)).astype(jnp.bfloat16)
    conv_rows = depthwise(gated_rows.reshape(-1, SEQ_LEN, local_channels), conv_taps).reshape(
        tok_rows, local_channels
    )
    channel_sum, channel_square = lax.psum(
        (jnp.sum(conv_rows, axis=1), jnp.sum(conv_rows * conv_rows, axis=1)), "tp"
    )
    row_mean = channel_sum / CA
    row_var = channel_square / CA - row_mean * row_mean
    activation = jax.nn.silu(
        (conv_rows - row_mean[:, None]) * lax.rsqrt(row_var + EPS)[:, None] * channel_gain
    ).astype(jnp.bfloat16)
    conv_term = jnp.dot(activation, mix_out, preferred_element_type=jnp.float32)
    attn_term = jnp.dot(attended, attn_out, preferred_element_type=jnp.float32)
    return lax.psum_scatter(
        (conv_term + blend_gain * attn_term).astype(jnp.bfloat16),
        "tp",
        scatter_dimension=0,
        tiled=True,
    )


BF = jnp.bfloat16
F32 = jnp.float32
NEG = -3e38


def mm(a, b):
    return jnp.dot(a, b, preferred_element_type=F32)


def wait_in(ref, sem):
    pltpu.make_async_copy(ref, ref, sem).wait()


def layer_kernel(
    n_st, n_tp, block_count, per_block, block_len, local_heads, seq_len, pass_rows,
    tokens_h, store_h, ids_v, mix_gain, gv_h, gg_h, taps, channel_gain, mo_h, query_gain,
    passage_gain, qw_h, kw_h, vw_h, ao_h, blend_gain,
    out_ref,
    tok, sto, gv, gg, mo, qw, kw, vw, ao, load_sem,
    ids_all, ids_s, ids_send, ids_recv, ids_sem,
    q_all, q_stage, q_send, q_recv,
    k_all, v_all, k_stage, v_stage, kv_send, kv_recv,
    gp, conv, scol, stat_all, stat_send, stat_recv, act,
    out_o, out_s, ret_o, ret_s, o_send, o_recv, s_send, s_recv, att,
    part, from_left, from_right, r_send, r_recv,
):
    st = lax.axis_index("st")
    tp = lax.axis_index("tp")
    core = lax.rem(st, 2)
    chip = st // 2
    n_chip = n_st // 2
    other = 1 - core
    T = tok.shape[0]
    R = sto.shape[0]
    HW = q_stage.shape[1]
    CL = act.shape[1]

    loads = []
    for n, (a, b) in enumerate(
        [(tokens_h, tok), (qw_h, qw), (gv_h, gv), (gg_h, gg), (store_h, sto), (kw_h, kw),
         (vw_h, vw), (mo_h, mo), (ao_h, ao)]
    ):
        c = pltpu.make_async_copy(a, b, load_sem.at[n])
        c.start()
        loads.append(c)

    barrier = pltpu.get_barrier_semaphore()
    for i in range(1, n_st):
        pl.semaphore_signal(barrier, inc=1, device_id={"st": lax.rem(st + i, n_st)},
                            device_id_type=pl.DeviceIdType.MESH)
    for i in range(1, n_tp):
        pl.semaphore_signal(barrier, inc=1, device_id={"tp": lax.rem(tp + i, n_tp)},
                            device_id_type=pl.DeviceIdType.MESH)

    def remote(src, dst, ssem, rsem, axis, to):
        return pltpu.make_async_remote_copy(
            src_ref=src, dst_ref=dst, send_sem=ssem, recv_sem=rsem, device_id={axis: to},
            device_id_type=pl.DeviceIdType.MESH)

    pl.semaphore_wait(barrier, n_st - 1 + n_tp - 1)

    for i in range(1, n_st):
        remote(ids_v, ids_all.at[st], ids_send.at[i], ids_recv.at[st], "st",
               lax.rem(st + i, n_st)).start()
    ids_own = pltpu.make_async_copy(ids_v, ids_all.at[st], ids_recv.at[st])
    ids_own.start()

    for n in range(4):
        loads[n].wait()
    TC = 256
    n_tc = T // TC
    per_seq = seq_len
    pad = (gp.shape[1] - per_seq) // 2
    gp[:, :pad] = jnp.zeros((gp.shape[0], pad, CL), F32)
    gp[:, pad + per_seq:] = jnp.zeros((gp.shape[0], pad, CL), F32)

    def peers():
        res = [(chip * 2 + other, True, 0)]
        for j in range(1, n_chip):
            c = lax.rem(chip + j, n_chip)
            res.append((c * 2 + core, False, 2 * j - 1))
            res.append((c * 2 + other, True, 2 * j))
        return res

    def tok_chunk(i, carry):
        rows = pl.ds(pl.multiple_of(i * TC, TC), TC)
        x = tok[rows, :].astype(F32)
        y = x * lax.rsqrt(jnp.mean(x * x, axis=-1, keepdims=True) + EPS)
        qr = (y * query_gain[...]).astype(BF)
        q_all[st, rows, :] = mm(qr, qw[:, pl.ds(pl.multiple_of(core * HW, HW), HW)]).astype(BF)
        q_stage[rows, :] = mm(qr, qw[:, pl.ds(pl.multiple_of(other * HW, HW), HW)]).astype(BF)
        for to, stage, n in peers():
            src = q_stage.at[rows] if stage else q_all.at[st, rows]
            remote(src, q_all.at[st, rows], q_send.at[n, i], q_recv.at[st, i], "st", to).start()
        mr = (y * mix_gain[...]).astype(BF)
        gated = (mm(mr, gv[...]) * jax.nn.sigmoid(mm(mr, gg[...]))).astype(BF).astype(F32)
        for u in range(TC // per_seq):
            gp[i * (TC // per_seq) + u, pad:pad + per_seq, :] = gated[u * per_seq:(u + 1) * per_seq]
        return carry

    lax.fori_loop(0, n_tc, tok_chunk, 0)

    for n in range(4, 7):
        loads[n].wait()
    RC = 256
    n_rc = R // RC
    RP = RC // pass_rows
    pass_local = R // pass_rows
    mine = pl.ds(pl.multiple_of(core * HW, HW), HW)
    theirs = pl.ds(pl.multiple_of(other * HW, HW), HW)
    partner = chip * 2 + other

    def store_chunk(i, carry):
        rows = pl.ds(pl.multiple_of(i * RC, RC), RC)
        x = sto[rows, :].astype(F32)
        n = (x * lax.rsqrt(jnp.mean(x * x, axis=-1, keepdims=True) + EPS) * passage_gain[...]).astype(BF)
        here, slots = pl.ds(i * RP, RP), pl.ds(core * pass_local + i * RP, RP)
        k_stage[here] = mm(n, kw[:, theirs]).astype(BF).reshape(RP, pass_rows, HW)
        v_stage[here] = mm(n, vw[:, theirs]).astype(BF).reshape(RP, pass_rows, HW)
        remote(k_stage.at[here], k_all.at[slots], kv_send.at[0, i], kv_recv.at[0, i], "st", partner).start()
        remote(v_stage.at[here], v_all.at[slots], kv_send.at[1, i], kv_recv.at[1, i], "st", partner).start()
        k_all[slots] = mm(n, kw[:, mine]).astype(BF).reshape(RP, pass_rows, HW)
        v_all[slots] = mm(n, vw[:, mine]).astype(BF).reshape(RP, pass_rows, HW)
        return carry

    lax.fori_loop(0, n_rc, store_chunk, 0)

    tap_values = taps[...].astype(F32)
    n_tap = taps.shape[0]
    lead = pad - (n_tap - 1) // 2
    CC = 32
    per = per_seq // CC
    lane = lax.broadcasted_iota(jnp.int32, (CC, 128), 1)

    def conv_chunk(i, carry):
        seq = i // per
        base = pl.multiple_of(lax.rem(i, per) * CC, CC)
        win = gp[seq, pl.ds(base, CC + 2 * pad), :]
        acc = jnp.zeros((CC, CL), F32)
        for k in range(n_tap):
            acc = acc + win[lead + k:lead + k + CC] * tap_values[k:k + 1]
        rows = pl.ds(pl.multiple_of(i * CC, CC), CC)
        conv[rows, :] = acc
        s = jnp.sum(acc, axis=1, keepdims=True)
        ss = jnp.sum(acc * acc, axis=1, keepdims=True)
        scol[rows, :] = jnp.where(lane == 0, s, jnp.where(lane == 1, ss, 0.0))
        return carry

    lax.fori_loop(0, T // CC, conv_chunk, 0)
    stat_all[tp] = jnp.transpose(scol[...])[:8]
    for i in range(1, n_tp):
        remote(stat_all.at[tp], stat_all.at[tp], stat_send.at[i], stat_recv.at[tp], "tp",
               lax.rem(tp + i, n_tp)).start()

    ids_own.wait()
    for i in range(1, n_st):
        r = lax.rem(st + i, n_st)
        remote(ids_v, ids_all.at[r], ids_send.at[i], ids_recv.at[r], "st", r).wait_recv()
    c = pltpu.make_async_copy(ids_all, ids_s, ids_sem)
    c.start()
    c.wait()

    def kv_wait(i, carry):
        here, slots = pl.ds(i * RP, RP), pl.ds(other * pass_local + i * RP, RP)
        remote(k_stage.at[here], k_all.at[slots], kv_send.at[0, i], kv_recv.at[0, i], "st", partner).wait()
        remote(v_stage.at[here], v_all.at[slots], kv_send.at[1, i], kv_recv.at[1, i], "st", partner).wait()
        return carry

    lax.fori_loop(0, n_rc, kv_wait, 0)

    heads = local_heads // 2
    HD_ = HW // heads
    per_chip = 2 * pass_local
    blane = lax.broadcasted_iota(jnp.int32, (block_len, 128), 1)
    scale = HD_ ** (-0.5)

    def order(i):
        return lax.rem(chip + 1 + i // 2, n_chip) * 2 + lax.rem(core + 1 - i % 2, 2)

    for i in range(n_st):
        r = order(i)
        own = i == n_st - 1
        if not own:
            def q_wait(j, carry, r=r):
                rows = pl.ds(pl.multiple_of(j * TC, TC), TC)
                remote(q_all.at[st, rows], q_all.at[r, rows], q_send.at[0, j], q_recv.at[r, j], "st", r).wait_recv()
                return carry
            lax.fori_loop(0, n_tc, q_wait, 0)

        def block(b, carry, r=r, own=own):
            rows = pl.ds(pl.multiple_of(b * block_len, block_len), block_len)
            stats = jnp.zeros((block_len, 128), F32)
            for h in range(heads):
                cols = slice(h * HD_, (h + 1) * HD_)
                q = q_all[r, rows, cols]
                tops, sums, outs, valids = [], [], [], []
                for j in range(per_block):
                    p = ids_s[r, b, j] - chip * per_chip
                    spread_p = jnp.full((block_len, 1), p, jnp.int32)
                    valid = jnp.logical_and(spread_p >= 0, spread_p < per_chip)
                    slot = jnp.clip(p, 0, per_chip - 1)
                    k = k_all[slot][:, cols]
                    v = v_all[slot][:, cols]
                    s = lax.dot_general(q, k, (((1,), (1,)), ((), ())), preferred_element_type=F32) * scale
                    top = jnp.max(s, axis=1, keepdims=True)
                    e = jnp.exp(s - top)
                    sums.append(jnp.sum(e, axis=1, keepdims=True))
                    outs.append(mm(e.astype(BF), v).astype(BF).astype(F32))
                    tops.append(jnp.where(valid, top, NEG))
                    valids.append(valid)
                best = functools.reduce(jnp.maximum, tops)
                num, den = 0.0, 0.0
                for j in range(per_block):
                    w = jnp.where(valids[j], jnp.exp(tops[j] - best), 0.0)
                    num = num + w * outs[j]
                    den = den + w * sums[j]
                if own:
                    ret_o[st, rows, cols] = num.astype(BF)
                else:
                    out_o[r, rows, cols] = num.astype(BF)
                stats = jnp.where(blane == 2 * h, best, jnp.where(blane == 2 * h + 1, den, stats))
            scol[rows, :] = stats
            return carry

        lax.fori_loop(0, block_count, block, 0)
        packed = jnp.transpose(scol[...])[:8]
        if own:
            ret_s[st] = packed
        else:
            out_s[r] = packed
            remote(out_o.at[r], ret_o.at[st], o_send.at[r], o_recv.at[st], "st", r).start()
            remote(out_s.at[r], ret_s.at[st], s_send.at[r], s_recv.at[st], "st", r).start()

    total = stat_all[tp]
    for i in range(1, n_tp):
        r = lax.rem(tp + i, n_tp)
        remote(stat_all.at[tp], stat_all.at[r], stat_send.at[i], stat_recv.at[r], "tp", r).wait_recv()
        total = total + stat_all[r]
    ca = CL * n_tp
    mean = total / ca
    spread = jnp.transpose(jnp.concatenate([mean, jnp.zeros((120, T), F32)], axis=0))
    row_mean = spread[:, 0:1]
    inv = lax.rsqrt(spread[:, 1:2] - row_mean * row_mean + EPS)
    a = (conv[...] - row_mean) * inv * channel_gain[...]
    act[...] = (a / (1.0 + jnp.exp(-a))).astype(BF)

    for i in range(n_st - 1):
        r = order(i)
        remote(out_o.at[r], ret_o.at[r], o_send.at[r], o_recv.at[r], "st", r).wait_recv()
        remote(out_s.at[r], ret_s.at[r], s_send.at[r], s_recv.at[r], "st", r).wait_recv()
    for g in range(2):
        cols_of = [jnp.transpose(jnp.concatenate([ret_s[c * 2 + g], jnp.zeros((120, T), F32)], axis=0))
                   for c in range(n_chip)]
        for h in range(heads):
            cols = slice(h * HD_, (h + 1) * HD_)
            best = functools.reduce(jnp.maximum, [x[:, 2 * h:2 * h + 1] for x in cols_of])
            num, den = 0.0, 0.0
            for c in range(n_chip):
                w = jnp.exp(cols_of[c][:, 2 * h:2 * h + 1] - best)
                num = num + w * ret_o[c * 2 + g, :, cols].astype(F32)
                den = den + w * cols_of[c][:, 2 * h + 1:2 * h + 2]
            att[:, g * HW + h * HD_:g * HW + (h + 1) * HD_] = (num / den).astype(BF)

    loads[7].wait()
    loads[8].wait()
    NC = 512
    n_nc = part.shape[1] // NC

    def out_cols(i, carry):
        cols = pl.ds(pl.multiple_of(i * NC, NC), NC)
        value = mm(act[...], mo[:, cols]) + blend_gain[:, cols] * mm(att[...], ao[:, cols])
        part[:, cols] = value.astype(BF)
        return carry

    lax.fori_loop(0, n_nc, out_cols, 0)

    rows_out = out_ref.shape[0]
    SUB = 4
    SR = rows_out // SUB

    def hop(d, u, ahead, buf, way, go, first, last):
        prow = pl.ds(pl.multiple_of(d * rows_out + u * SR, SR), SR)
        brow = pl.ds(u * SR, SR)
        to = jnp.clip(tp + ahead, 0, n_tp - 1)
        copy = remote(part.at[prow], buf.at[d, brow], r_send.at[way, d, u], r_recv.at[way, d, u], "tp", to)

        @pl.when(jnp.logical_and(go, jnp.logical_not(first)))
        def _():
            copy.wait_recv()
            part[prow, :] = (part[prow, :].astype(F32) + buf[d, brow, :].astype(F32)).astype(BF)

        @pl.when(go)
        def _():
            copy.start()

    for i in range(1, n_tp):
        for u in range(SUB):
            d = n_tp - i
            hop(d, u, 1, from_left, 0, tp < d, tp == 0, None)
            d = i - 1
            hop(d, u, -1, from_right, 1, tp > d, tp == n_tp - 1, None)

    for u in range(SUB):
        prow = pl.ds(pl.multiple_of(tp * rows_out + u * SR, SR), SR)
        brow = pl.ds(u * SR, SR)
        out_acc = part[prow, :].astype(F32)
        conv_rows = brow

        @pl.when(tp > 0)
        def _():
            remote(part.at[prow], from_left.at[tp, brow], r_send.at[0, tp, u], r_recv.at[0, tp, u], "tp",
                   jnp.maximum(tp - 1, 0)).wait_recv()

        @pl.when(tp == 0)
        def _():
            from_left[0, brow, :] = jnp.zeros((SR, part.shape[1]), BF)

        @pl.when(tp < n_tp - 1)
        def _():
            remote(part.at[prow], from_right.at[tp, brow], r_send.at[1, tp, u], r_recv.at[1, tp, u], "tp",
                   jnp.minimum(tp + 1, n_tp - 1)).wait_recv()

        @pl.when(tp == n_tp - 1)
        def _():
            from_right[n_tp - 1, brow, :] = jnp.zeros((SR, part.shape[1]), BF)

        out_ref[brow, :] = (
            out_acc + from_left[tp, brow, :].astype(F32) + from_right[tp, brow, :].astype(F32)
        ).astype(BF)

    for i in range(1, n_st):
        r = lax.rem(st + i, n_st)
        remote(ids_v, ids_all.at[st], ids_send.at[i], ids_recv.at[st], "st", r).wait_send()
    for i in range(n_tc):
        rows = pl.ds(i * TC, TC)
        for to, stage, n in peers():
            src = q_stage.at[rows] if stage else q_all.at[st, rows]
            remote(src, q_all.at[st, rows], q_send.at[n, i], q_recv.at[st, i], "st", to).wait_send()
    for i in range(1, n_tp):
        remote(stat_all.at[tp], stat_all.at[tp], stat_send.at[i], stat_recv.at[tp], "tp",
               lax.rem(tp + i, n_tp)).wait_send()
    for i in range(n_st - 1):
        r = order(i)
        remote(out_o.at[r], ret_o.at[st], o_send.at[r], o_recv.at[st], "st", r).wait_send()
        remote(out_s.at[r], ret_s.at[st], s_send.at[r], s_recv.at[st], "st", r).wait_send()
    for d in range(n_tp):
        for u in range(SUB):
            prow = pl.ds(d * rows_out + u * SR, SR)

            @pl.when(tp < d)
            def _():
                remote(part.at[prow], from_left.at[d, pl.ds(u * SR, SR)], r_send.at[0, d, u],
                       r_recv.at[0, d, u], "tp", jnp.minimum(tp + 1, n_tp - 1)).wait_send()

            @pl.when(tp > d)
            def _():
                remote(part.at[prow], from_right.at[d, pl.ds(u * SR, SR)], r_send.at[1, d, u],
                       r_recv.at[1, d, u], "tp", jnp.maximum(tp - 1, 0)).wait_send()


def fused_local(
    tokens, store, passage_ids, mix_gain, glu_value, glu_gate, conv_taps, channel_gain, mix_out,
    query_gain, passage_gain, query_proj, key_proj, value_proj, attn_out, blend_gain,
):
    n_st = lax.axis_size("st")
    n_tp = lax.axis_size("tp")
    T, D = tokens.shape
    P_, PR, _ = store.shape
    R = P_ * PR
    W = query_proj.shape[1]
    HW = W // 2
    CL = glu_value.shape[1]
    nb, per_block = passage_ids.shape
    ids = jnp.pad(passage_ids, ((0, 0), (0, 128 - per_block)))
    pad = 8 * pl.cdiv((conv_taps.shape[0] - 1) // 2, 8)
    DMA = pltpu.SemaphoreType.DMA
    V = pltpu.VMEM
    SUB = 4
    kern = functools.partial(layer_kernel, n_st, n_tp, nb, per_block, T // nb, W // HD, SEQ_LEN, PR)
    hbm = pl.BlockSpec(memory_space=pl.ANY)
    vm = pl.BlockSpec(memory_space=pltpu.VMEM)
    return pl.pallas_call(
        kern,
        out_shape=jax.ShapeDtypeStruct((T // n_tp, D), BF),
        in_specs=[hbm, hbm, vm, vm, hbm, hbm, vm, vm, hbm, vm, vm, hbm, hbm, hbm, hbm, vm],
        out_specs=vm,
        scratch_shapes=[
            V((T, D), BF), V((R, D), BF), V((D, CL), BF), V((D, CL), BF), V((CL, D), BF),
            V((D, W), BF), V((D, W), BF), V((D, W), BF), V((W, D), BF), DMA((9,)),
            V((n_st, nb, 128), jnp.int32), pltpu.SMEM((n_st, nb, 128), jnp.int32),
            DMA((n_st,)), DMA((n_st,)), DMA,
            V((n_st, T, HW), BF), V((T, HW), BF), DMA((n_st - 1, T // 256)), DMA((n_st, T // 256)),
            V((2 * P_, PR, HW), BF), V((2 * P_, PR, HW), BF), V((P_, PR, HW), BF), V((P_, PR, HW), BF),
            DMA((2, R // 256)), DMA((2, R // 256)),
            V((T // SEQ_LEN, SEQ_LEN + 2 * pad, CL), F32), V((T, CL), F32), V((T, 128), F32),
            V((n_tp, 8, T), F32), DMA((n_tp,)), DMA((n_tp,)), V((T, CL), BF),
            V((n_st, T, HW), BF), V((n_st, 8, T), F32), V((n_st, T, HW), BF), V((n_st, 8, T), F32),
            DMA((n_st,)), DMA((n_st,)), DMA((n_st,)), DMA((n_st,)), V((T, W), BF),
            V((T, D), BF), V((n_tp, T // n_tp, D), BF), V((n_tp, T // n_tp, D), BF),
            DMA((2, n_tp, SUB)), DMA((2, n_tp, SUB)),
        ],
        compiler_params=pltpu.CompilerParams(
            collective_id=0, has_side_effects=True, vmem_limit_bytes=60 * 1024 * 1024),
        name="layer",
    )(
        tokens, store.reshape(R, D), ids, mix_gain.reshape(1, D), glu_value, glu_gate, conv_taps,
        channel_gain.reshape(1, CL), mix_out, query_gain.reshape(1, D), passage_gain.reshape(1, D),
        query_proj, key_proj, value_proj, attn_out, blend_gain.reshape(1, D),
    )


def solution(mesh):
    in_specs = (
        P(("grp", "st"), None),
        P(("grp", "st"), None, None),
        P(("grp", "st"), None),
        P(),
        P(None, "tp"),
        P(None, "tp"),
        P(None, "tp"),
        P("tp"),
        P("tp", None),
        P(),
        P(),
        P(None, "tp"),
        P(None, "tp"),
        P(None, "tp"),
        P("tp", None),
        P(),
    )
    out_specs = P(("grp", "st", "tp"), None)
    def body(*args):
        even = args[11].shape[1] // HD % 2 == 0 and mesh.shape["st"] % 2 == 0
        return (fused_local if even else local)(*args)

    return jax.shard_map(body, mesh=mesh, in_specs=in_specs, out_specs=out_specs, check_vma=False)
```

```python
import functools

import jax
import jax.numpy as jnp
from jax import lax
from jax.sharding import PartitionSpec as P
from jax.experimental import pallas as pl
from jax.experimental.pallas import tpu as pltpu

CA = 1024
HD = 256
SEQ_LEN = 128


EPS = 1e-06


def rms_rows(row_data, gain_vec):
    floats = row_data.astype(jnp.float32)
    inv_scale = lax.rsqrt(jnp.mean(floats * floats, axis=-1, keepdims=True) + EPS)
    return (floats * inv_scale * gain_vec).astype(jnp.bfloat16)


def depthwise(gated_rows, conv_taps):
    span_width = conv_taps.shape[0]
    half_span = (span_width - 1) // 2
    seq_length = gated_rows.shape[1]
    padded = jnp.pad(
        gated_rows.astype(jnp.float32), ((0, 0), (half_span, span_width - 1 - half_span), (0, 0))
    )
    running = jnp.zeros(gated_rows.shape, jnp.float32)
    for tap_index in range(span_width):
        running = running + padded[:, tap_index : tap_index + seq_length] * conv_taps[
            tap_index
        ].astype(jnp.float32)
    return running


def passage_attention(queries, keys_values, head_count):
    groups, block_len, span_width = queries.shape
    head_dim = span_width // head_count
    row_count = keys_values.shape[1]
    query_heads = queries.reshape(groups, block_len, head_count, head_dim)
    key_heads = keys_values[:, :, :span_width].reshape(groups, row_count, head_count, head_dim)
    value_heads = keys_values[:, :, span_width:].reshape(groups, row_count, head_count, head_dim)
    scores = jnp.einsum(
        "gqhd,grhd->ghqr", query_heads, key_heads, preferred_element_type=jnp.float32
    ) * head_dim ** (-0.5)
    row_top = jnp.max(scores, axis=-1)
    exponent = jnp.exp(scores - row_top[..., None])
    row_sum = jnp.sum(exponent, axis=-1)
    weights = exponent.astype(jnp.bfloat16)
    outputs = jnp.einsum(
        "ghqr,grhd->gqhd", weights, value_heads, preferred_element_type=jnp.float32
    ).astype(jnp.bfloat16)
    return (outputs.reshape(groups, block_len, span_width), row_top, row_sum)


def combine(outs, tops, sums, head_count):
    batch_count, passage_count, block_len, span_width = outs.shape
    head_dim = span_width // head_count
    best_top = jnp.max(tops, axis=1, keepdims=True)
    weight = jnp.exp(tops - best_top)
    numerator = jnp.einsum(
        "bphq,bpqhd->bqhd",
        weight,
        outs.astype(jnp.float32).reshape(
            batch_count, passage_count, block_len, head_count, head_dim
        ),
    )
    denominator = jnp.sum(weight * sums, axis=1)
    result = numerator / jnp.transpose(denominator, (0, 2, 1))[..., None]
    return result.reshape(batch_count, block_len, span_width).astype(jnp.bfloat16)


def local(
    tokens,
    store,
    passage_ids,
    mix_gain,
    glu_value,
    glu_gate,
    conv_taps,
    channel_gain,
    mix_out,
    query_gain,
    passage_gain,
    query_proj,
    key_proj,
    value_proj,
    attn_out,
    blend_gain,
):
    owners = lax.axis_size("st")
    tok_rows = tokens.shape[0]
    model_width = tokens.shape[1]
    local_channels = glu_value.shape[1]
    head_width = query_proj.shape[1]
    local_heads = head_width // HD
    block_count = passage_ids.shape[0]
    per_block = passage_ids.shape[1]
    block_len = tok_rows // block_count
    requests = block_count * per_block
    capacity = 2 * requests // owners
    pass_local = store.shape[0]
    pass_rows = store.shape[1]
    flat_ids = passage_ids.reshape(requests)
    owner_of = flat_ids // pass_local
    local_of = flat_ids - owner_of * pass_local
    request_index = jnp.arange(requests)
    earlier = (owner_of[:, None] == owner_of[None, :]) & (
        request_index[None, :] < request_index[:, None]
    )
    ranking = jnp.sum(earlier.astype(jnp.int32), axis=1)
    slot_of = owner_of * capacity + ranking
    slot_ids = (
        jnp.zeros((owners * capacity,), jnp.int32)
        .at[slot_of]
        .set(local_of)
        .reshape(owners, capacity)
    )
    asked = lax.all_to_all(slot_ids, "st", split_axis=0, concat_axis=0, tiled=True)
    normed_store = rms_rows(store.reshape(pass_local * pass_rows, model_width), passage_gain)
    key_rows = jnp.dot(normed_store, key_proj, preferred_element_type=jnp.float32).astype(
        jnp.bfloat16
    )
    value_rows = jnp.dot(normed_store, value_proj, preferred_element_type=jnp.float32).astype(
        jnp.bfloat16
    )
    memory = jnp.concatenate([key_rows, value_rows], axis=1).reshape(
        pass_local, pass_rows, 2 * head_width
    )
    queries = jnp.dot(
        rms_rows(tokens, query_gain), query_proj, preferred_element_type=jnp.float32
    ).astype(jnp.bfloat16)
    query_blocks = queries.reshape(block_count, block_len, head_width)
    repeated = jnp.repeat(query_blocks, per_block, axis=0)
    served = memory[asked.reshape(owners * capacity)]
    slot_queries = (
        jnp.zeros((owners * capacity, block_len, head_width), jnp.bfloat16)
        .at[slot_of]
        .set(repeated)
    )
    visiting = lax.all_to_all(
        slot_queries.reshape(owners, capacity, block_len, head_width),
        "st",
        split_axis=0,
        concat_axis=0,
        tiled=True,
    )
    answer_out, answer_top, answer_sum = passage_attention(
        visiting.reshape(owners * capacity, block_len, head_width), served, local_heads
    )
    back_out = lax.all_to_all(
        answer_out.reshape(owners, capacity, block_len, head_width),
        "st",
        split_axis=0,
        concat_axis=0,
        tiled=True,
    )
    back_top, back_sum = (
        lax.all_to_all(
            answer_top.reshape(owners, capacity, local_heads, block_len),
            "st",
            split_axis=0,
            concat_axis=0,
            tiled=True,
        ),
        lax.all_to_all(
            answer_sum.reshape(owners, capacity, local_heads, block_len),
            "st",
            split_axis=0,
            concat_axis=0,
            tiled=True,
        ),
    )
    partial_out = back_out.reshape(owners * capacity, block_len, head_width)[slot_of]
    partial_top = back_top.reshape(owners * capacity, local_heads, block_len)[slot_of]
    partial_sum = back_sum.reshape(owners * capacity, local_heads, block_len)[slot_of]
    attended = combine(
        partial_out.reshape(block_count, per_block, block_len, head_width),
        partial_top.reshape(block_count, per_block, local_heads, block_len),
        partial_sum.reshape(block_count, per_block, local_heads, block_len),
        local_heads,
    ).reshape(tok_rows, head_width)
    mix_input = rms_rows(tokens, mix_gain)
    value_part = jnp.dot(mix_input, glu_value, preferred_element_type=jnp.float32)
    gate_part = jnp.dot(mix_input, glu_gate, preferred_element_type=jnp.float32)
    gated_rows = (value_part * jax.nn.sigmoid(gate_part)).astype(jnp.bfloat16)
    conv_rows = depthwise(gated_rows.reshape(-1, SEQ_LEN, local_channels), conv_taps).reshape(
        tok_rows, local_channels
    )
    channel_sum, channel_square = lax.psum(
        (jnp.sum(conv_rows, axis=1), jnp.sum(conv_rows * conv_rows, axis=1)), "tp"
    )
    row_mean = channel_sum / CA
    row_var = channel_square / CA - row_mean * row_mean
    activation = jax.nn.silu(
        (conv_rows - row_mean[:, None]) * lax.rsqrt(row_var + EPS)[:, None] * channel_gain
    ).astype(jnp.bfloat16)
    conv_term = jnp.dot(activation, mix_out, preferred_element_type=jnp.float32)
    attn_term = jnp.dot(attended, attn_out, preferred_element_type=jnp.float32)
    return lax.psum_scatter(
        (conv_term + blend_gain * attn_term).astype(jnp.bfloat16),
        "tp",
        scatter_dimension=0,
        tiled=True,
    )


BF = jnp.bfloat16
F32 = jnp.float32
NEG = -3e38


def mm(a, b):
    return jnp.dot(a, b, preferred_element_type=F32)


def wait_in(ref, sem):
    pltpu.make_async_copy(ref, ref, sem).wait()


def layer_kernel(
    n_st, n_tp, block_count, per_block, block_len, local_heads, seq_len, pass_rows,
    tokens_h, store_h, ids_v, mix_gain, gv_h, gg_h, taps, channel_gain, mo_h, query_gain,
    passage_gain, qw_h, kw_h, vw_h, ao_h, blend_gain,
    out_ref,
    tok, sto, gv, gg, mo, qw, kw, vw, ao, load_sem,
    ids_all, ids_s, ids_send, ids_recv, ids_sem,
    q_all, q_stage, q_send, q_recv,
    k_all, v_all, k_stage, v_stage, kv_send, kv_recv,
    gp, conv, scol, stat_all, stat_send, stat_recv, act,
    out_o, out_s, ret_o, ret_s, o_send, o_recv, s_send, s_recv,
    part, from_left, from_right, r_send, r_recv,
):
    st = lax.axis_index("st")
    tp = lax.axis_index("tp")
    core = lax.rem(st, 2)
    chip = st // 2
    n_chip = n_st // 2
    other = 1 - core
    T = tok.shape[0]
    R = sto.shape[0]
    HW = q_stage.shape[1]
    CL = act.shape[1]

    loads = []
    for n, (a, b) in enumerate(
        [(tokens_h, tok), (qw_h, qw), (store_h, sto), (kw_h, kw), (vw_h, vw), (gv_h, gv),
         (gg_h, gg), (mo_h, mo), (ao_h, ao)]
    ):
        c = pltpu.make_async_copy(a, b, load_sem.at[n])
        c.start()
        loads.append(c)

    barrier = pltpu.get_barrier_semaphore()
    for i in range(1, n_st):
        pl.semaphore_signal(barrier, inc=1, device_id={"st": lax.rem(st + i, n_st)},
                            device_id_type=pl.DeviceIdType.MESH)
    for i in range(1, n_tp):
        pl.semaphore_signal(barrier, inc=1, device_id={"tp": lax.rem(tp + i, n_tp)},
                            device_id_type=pl.DeviceIdType.MESH)

    def remote(src, dst, ssem, rsem, axis, to):
        return pltpu.make_async_remote_copy(
            src_ref=src, dst_ref=dst, send_sem=ssem, recv_sem=rsem, device_id={axis: to},
            device_id_type=pl.DeviceIdType.MESH)

    chunk_rows = T // n_tp
    table = [sorted(range(n_tp), key=lambda d: -abs(d - t)) for t in range(n_tp)]

    def chunk_at(k):
        d = jnp.int32(table[0][k])
        for t in range(1, n_tp):
            d = jnp.where(tp == t, table[t][k], d)
        return d

    chunks = [chunk_at(k) for k in range(n_tp)]

    def chunk_ds(d):
        return pl.ds(pl.multiple_of(d * chunk_rows, chunk_rows), chunk_rows)

    def peers():
        res = [(chip * 2 + other, True, 0)]
        for j in range(1, n_chip):
            c = lax.rem(chip + j, n_chip)
            res.append((c * 2 + core, False, 2 * j - 1))
            res.append((c * 2 + other, True, 2 * j))
        return res

    loads[0].wait()
    loads[1].wait()
    TC = 256
    mine = pl.ds(pl.multiple_of(core * HW, HW), HW)
    theirs = pl.ds(pl.multiple_of(other * HW, HW), HW)

    def tok_chunk(i, carry):
        rows = pl.ds(pl.multiple_of(i * TC, TC), TC)
        x = tok[rows, :].astype(F32)
        y = x * lax.rsqrt(jnp.mean(x * x, axis=-1, keepdims=True) + EPS)
        qr = (y * query_gain[...]).astype(BF)
        q_all[st, rows, :] = mm(qr, qw[:, mine]).astype(BF)
        q_stage[rows, :] = mm(qr, qw[:, theirs]).astype(BF)
        tok[rows, :] = (y * mix_gain[...]).astype(BF)
        return carry

    lax.fori_loop(0, T // TC, tok_chunk, 0)

    pl.semaphore_wait(barrier, n_st - 1 + n_tp - 1)
    for i in range(1, n_st):
        remote(ids_v, ids_all.at[st], ids_send.at[i], ids_recv.at[st], "st",
               lax.rem(st + i, n_st)).start()
    ids_own = pltpu.make_async_copy(ids_v, ids_all.at[st], ids_recv.at[st])
    ids_own.start()

    def q_copies(k):
        rows = chunk_ds(chunks[k])
        for to, stage, n in peers():
            src = q_stage.at[rows] if stage else q_all.at[st, rows]
            yield remote(src, q_all.at[st, rows], q_send.at[n, k], q_recv.at[st, k], "st", to)

    for k in range(n_tp):
        for c in q_copies(k):
            c.start()

    for n in range(2, 5):
        loads[n].wait()
    RC = 256
    n_rc = R // RC
    RP = RC // pass_rows
    pass_local = R // pass_rows
    partner = chip * 2 + other

    def store_chunk(i, carry):
        rows = pl.ds(pl.multiple_of(i * RC, RC), RC)
        x = sto[rows, :].astype(F32)
        n = (x * lax.rsqrt(jnp.mean(x * x, axis=-1, keepdims=True) + EPS) * passage_gain[...]).astype(BF)
        here, slots = pl.ds(i * RP, RP), pl.ds(core * pass_local + i * RP, RP)
        k_stage[here] = mm(n, kw[:, theirs]).astype(BF).reshape(RP, pass_rows, HW)
        v_stage[here] = mm(n, vw[:, theirs]).astype(BF).reshape(RP, pass_rows, HW)
        remote(k_stage.at[here], k_all.at[slots], kv_send.at[0, i], kv_recv.at[0, i], "st", partner).start()
        remote(v_stage.at[here], v_all.at[slots], kv_send.at[1, i], kv_recv.at[1, i], "st", partner).start()
        k_all[slots] = mm(n, kw[:, mine]).astype(BF).reshape(RP, pass_rows, HW)
        v_all[slots] = mm(n, vw[:, mine]).astype(BF).reshape(RP, pass_rows, HW)
        return carry

    lax.fori_loop(0, n_rc, store_chunk, 0)

    ids_own.wait()
    for i in range(1, n_st):
        r = lax.rem(st + i, n_st)
        remote(ids_v, ids_all.at[r], ids_send.at[i], ids_recv.at[r], "st", r).wait_recv()
    c = pltpu.make_async_copy(ids_all, ids_s, ids_sem)
    c.start()
    c.wait()

    def kv_wait(i, carry):
        here, slots = pl.ds(i * RP, RP), pl.ds(other * pass_local + i * RP, RP)
        remote(k_stage.at[here], k_all.at[slots], kv_send.at[0, i], kv_recv.at[0, i], "st", partner).wait()
        remote(v_stage.at[here], v_all.at[slots], kv_send.at[1, i], kv_recv.at[1, i], "st", partner).wait()
        return carry

    lax.fori_loop(0, n_rc, kv_wait, 0)

    heads = local_heads // 2
    HD_ = HW // heads
    per_chip = 2 * pass_local
    chunk_blocks = block_count // n_tp
    clane = lax.broadcasted_iota(jnp.int32, (chunk_rows, 128), 1)
    scale = HD_ ** (-0.5)

    def order(i):
        return lax.rem(chip + 1 + i // 2, n_chip) * 2 + lax.rem(core + 1 - i % 2, 2)

    def answer_copies(k, r):
        rows = chunk_ds(chunks[k])
        return (
            remote(out_o.at[r, rows], ret_o.at[st, rows], o_send.at[r, k], o_recv.at[st, k], "st", r),
            remote(out_s.at[r, k], ret_s.at[st, k], s_send.at[r, k], s_recv.at[st, k], "st", r),
        )

    def attend(k):
        d = chunks[k]
        rows = chunk_ds(d)

        def one(i, carry):
            r = order(i)

            @pl.when(i < n_st - 1)
            def _():
                remote(q_all.at[st, rows], q_all.at[r, rows], q_send.at[0, k], q_recv.at[r, k], "st", r).wait_recv()

            stats = jnp.zeros((chunk_rows, 128), F32)
            for h in range(heads):
                cols = slice(h * HD_, (h + 1) * HD_)
                tops, dens = [], []
                for u in range(chunk_blocks):
                    b = d * chunk_blocks + u
                    brow = pl.ds(pl.multiple_of(b * block_len, block_len), block_len)
                    q = q_all[r, brow, cols]
                    ks, vs, bias = [], [], []
                    for j in range(per_block):
                        p = ids_s[r, b, j] - chip * per_chip
                        spread_p = jnp.full((1, pass_rows), p, jnp.int32)
                        valid = jnp.logical_and(spread_p >= 0, spread_p < per_chip)
                        bias.append(jnp.where(valid, 0.0, NEG))
                        slot = jnp.clip(p, 0, per_chip - 1)
                        ks.append(k_all[slot][:, cols])
                        vs.append(v_all[slot][:, cols])
                    s = lax.dot_general(q, jnp.concatenate(ks, axis=0), (((1,), (1,)), ((), ())),
                                        preferred_element_type=F32)
                    s = s * scale + jnp.concatenate(bias, axis=1)
                    top = jnp.maximum(jnp.max(s, axis=1, keepdims=True), NEG / 2)
                    e = jnp.exp(s - top)
                    dens.append(jnp.sum(e, axis=1, keepdims=True))
                    tops.append(top)
                    out_o[r, brow, cols] = mm(e.astype(BF), jnp.concatenate(vs, axis=0)).astype(BF)
                stats = jnp.where(clane == 2 * h, jnp.concatenate(tops, axis=0), stats)
                stats = jnp.where(clane == 2 * h + 1, jnp.concatenate(dens, axis=0), stats)
            out_s[r, k] = jnp.transpose(stats)[:8]

            @pl.when(i < n_st - 1)
            def _():
                for c in answer_copies(k, r):
                    c.start()

            return carry

        lax.fori_loop(0, n_st, one, 0)

    attend(0)

    loads[5].wait()
    loads[6].wait()
    per_seq = seq_len
    pad = (gp.shape[1] - per_seq) // 2
    gp[:, :pad] = jnp.zeros((gp.shape[0], pad, CL), F32)
    gp[:, pad + per_seq:] = jnp.zeros((gp.shape[0], pad, CL), F32)

    def glu_chunk(i, carry):
        mr = tok[pl.ds(pl.multiple_of(i * TC, TC), TC), :]
        gated = (mm(mr, gv[...]) * jax.nn.sigmoid(mm(mr, gg[...]))).astype(BF).astype(F32)
        for u in range(TC // per_seq):
            gp[i * (TC // per_seq) + u, pad:pad + per_seq, :] = gated[u * per_seq:(u + 1) * per_seq]
        return carry

    lax.fori_loop(0, T // TC, glu_chunk, 0)
    tap_values = taps[...].astype(F32)
    n_tap = taps.shape[0]
    lead = pad - (n_tap - 1) // 2
    CC = 32
    per = per_seq // CC
    lane = lax.broadcasted_iota(jnp.int32, (CC, 128), 1)

    def conv_chunk(i, carry):
        seq = i // per
        base = pl.multiple_of(lax.rem(i, per) * CC, CC)
        win = gp[seq, pl.ds(base, CC + 2 * pad), :]
        acc = jnp.zeros((CC, CL), F32)
        for k in range(n_tap):
            acc = acc + win[lead + k:lead + k + CC] * tap_values[k:k + 1]
        rows = pl.ds(pl.multiple_of(i * CC, CC), CC)
        conv[rows, :] = acc
        s = jnp.sum(acc, axis=1, keepdims=True)
        ss = jnp.sum(acc * acc, axis=1, keepdims=True)
        scol[rows, :] = jnp.where(lane == 0, s, jnp.where(lane == 1, ss, 0.0))
        return carry

    lax.fori_loop(0, T // CC, conv_chunk, 0)
    stat_all[tp] = jnp.transpose(scol[...])[:8]
    for i in range(1, n_tp):
        remote(stat_all.at[tp], stat_all.at[tp], stat_send.at[i], stat_recv.at[tp], "tp",
               lax.rem(tp + i, n_tp)).start()

    attend(1)

    total = stat_all[tp]
    for i in range(1, n_tp):
        r = lax.rem(tp + i, n_tp)
        remote(stat_all.at[tp], stat_all.at[r], stat_send.at[i], stat_recv.at[r], "tp", r).wait_recv()
        total = total + stat_all[r]
    ca = CL * n_tp
    mean = total / ca
    spread = jnp.transpose(jnp.concatenate([mean, jnp.zeros((120, T), F32)], axis=0))
    row_mean = spread[:, 0:1]
    inv = lax.rsqrt(spread[:, 1:2] - row_mean * row_mean + EPS)
    a = (conv[...] - row_mean) * inv * channel_gain[...]
    act[...] = (a / (1.0 + jnp.exp(-a))).astype(BF)
    loads[7].wait()
    loads[8].wait()

    SUB = 4
    SR = chunk_rows // SUB

    def hop(k, u, ahead, buf, way):
        d = chunks[k]
        prow = pl.ds(pl.multiple_of(d * chunk_rows + u * SR, SR), SR)
        brow = pl.ds(u * SR, SR)
        to = jnp.clip(tp + ahead, 0, n_tp - 1)
        return prow, brow, remote(part.at[prow], buf.at[d, brow], r_send.at[way, d, u],
                                  r_recv.at[way, d, u], "tp", to)

    ways = ((1, from_left, 0), (-1, from_right, 1))

    def goes(k, way):
        return tp < chunks[k] if way == 0 else tp > chunks[k]

    def at_end(way):
        return tp == 0 if way == 0 else tp == n_tp - 1

    def finish(k):
        rows = chunk_ds(chunks[k])
        for i in range(n_st - 1):
            r = order(i)
            remote(out_o.at[r, rows], ret_o.at[r, rows], o_send.at[r, k], o_recv.at[r, k], "st", r).wait_recv()
            remote(out_s.at[r, k], ret_s.at[r, k], s_send.at[r, k], s_recv.at[r, k], "st", r).wait_recv()
        ret_o[st, rows, :] = out_o[st, rows, :]
        ret_s[st, k] = out_s[st, k]
        stats = jnp.transpose(jnp.concatenate(
            [ret_s[c, k] for c in range(n_st)] + [jnp.zeros((128 - 8 * n_st, chunk_rows), F32)], axis=0))
        pieces = []
        for g in range(2):
            for h in range(heads):
                cols = slice(h * HD_, (h + 1) * HD_)
                at = [8 * (c * 2 + g) + 2 * h for c in range(n_chip)]
                best = functools.reduce(jnp.maximum, [stats[:, x:x + 1] for x in at])
                num, den = 0.0, 0.0
                for c in range(n_chip):
                    w = jnp.exp(stats[:, at[c]:at[c] + 1] - best)
                    num = num + w * ret_o[c * 2 + g, rows, cols].astype(F32)
                    den = den + w * stats[:, at[c] + 1:at[c] + 2]
                pieces.append((num / den).astype(BF))
        attended = jnp.concatenate(pieces, axis=1)
        act_rows = act[rows, :]
        NC = 512
        for i in range(part.shape[1] // NC):
            cols = slice(i * NC, (i + 1) * NC)
            value = mm(act_rows, mo[:, cols]) + blend_gain[:, cols] * mm(attended, ao[:, cols])
            part[rows, cols] = value.astype(BF)
        if k < n_tp - 1:
            for ahead, buf, way in ways:
                @pl.when(jnp.logical_and(goes(k, way), at_end(way)))
                def _(ahead=ahead, buf=buf, way=way):
                    for u in range(SUB):
                        hop(k, u, ahead, buf, way)[2].start()

    def forward(k, u):
        for ahead, buf, way in ways:
            @pl.when(jnp.logical_and(goes(k, way), jnp.logical_not(at_end(way))))
            def _(ahead=ahead, buf=buf, way=way):
                prow, brow, copy = hop(k, u, ahead, buf, way)
                copy.wait_recv()
                part[prow, :] = (part[prow, :].astype(F32) + buf[chunks[k], brow, :].astype(F32)).astype(BF)
                copy.start()

    forwarded = 0
    for k in range(n_tp):
        finish(k)
        if k + 2 < n_tp:
            attend(k + 2)
        elif k < n_tp - 1:
            for u in range(SUB):
                forward(k - 2, u)
            forwarded = k - 1
    for u in range(SUB):
        for k in range(forwarded, n_tp - 1):
            forward(k, u)

    for u in range(SUB):
        prow = pl.ds(pl.multiple_of(tp * chunk_rows + u * SR, SR), SR)
        brow = pl.ds(u * SR, SR)

        for ahead, buf, way in ways:
            @pl.when(jnp.logical_not(at_end(way)))
            def _(buf=buf, way=way, ahead=ahead):
                to = jnp.clip(tp - ahead, 0, n_tp - 1)
                remote(part.at[prow], buf.at[tp, brow], r_send.at[way, tp, u], r_recv.at[way, tp, u], "tp",
                       to).wait_recv()

            @pl.when(at_end(way))
            def _(buf=buf):
                buf[tp, brow, :] = jnp.zeros((SR, part.shape[1]), BF)

        out_ref[brow, :] = (
            part[prow, :].astype(F32) + from_left[tp, brow, :].astype(F32) + from_right[tp, brow, :].astype(F32)
        ).astype(BF)

    for i in range(1, n_st):
        r = lax.rem(st + i, n_st)
        remote(ids_v, ids_all.at[st], ids_send.at[i], ids_recv.at[st], "st", r).wait_send()
    for k in range(n_tp):
        for c in q_copies(k):
            c.wait_send()
        for i in range(n_st - 1):
            for c in answer_copies(k, order(i)):
                c.wait_send()
    for i in range(1, n_tp):
        remote(stat_all.at[tp], stat_all.at[tp], stat_send.at[i], stat_recv.at[tp], "tp",
               lax.rem(tp + i, n_tp)).wait_send()
    for k in range(n_tp - 1):
        for ahead, buf, way in ways:
            @pl.when(goes(k, way))
            def _(ahead=ahead, buf=buf, way=way):
                for u in range(SUB):
                    hop(k, u, ahead, buf, way)[2].wait_send()


def fused_local(
    tokens, store, passage_ids, mix_gain, glu_value, glu_gate, conv_taps, channel_gain, mix_out,
    query_gain, passage_gain, query_proj, key_proj, value_proj, attn_out, blend_gain,
):
    n_st = lax.axis_size("st")
    n_tp = lax.axis_size("tp")
    T, D = tokens.shape
    P_, PR, _ = store.shape
    R = P_ * PR
    W = query_proj.shape[1]
    HW = W // 2
    CL = glu_value.shape[1]
    nb, per_block = passage_ids.shape
    ids = jnp.pad(passage_ids, ((0, 0), (0, 128 - per_block)))
    pad = 8 * pl.cdiv((conv_taps.shape[0] - 1) // 2, 8)
    DMA = pltpu.SemaphoreType.DMA
    V = pltpu.VMEM
    SUB = 4
    kern = functools.partial(layer_kernel, n_st, n_tp, nb, per_block, T // nb, W // HD, SEQ_LEN, PR)
    hbm = pl.BlockSpec(memory_space=pl.ANY)
    vm = pl.BlockSpec(memory_space=pltpu.VMEM)
    return pl.pallas_call(
        kern,
        out_shape=jax.ShapeDtypeStruct((T // n_tp, D), BF),
        in_specs=[hbm, hbm, vm, vm, hbm, hbm, vm, vm, hbm, vm, vm, hbm, hbm, hbm, hbm, vm],
        out_specs=vm,
        scratch_shapes=[
            V((T, D), BF), V((R, D), BF), V((D, CL), BF), V((D, CL), BF), V((CL, D), BF),
            V((D, W), BF), V((D, W), BF), V((D, W), BF), V((W, D), BF), DMA((9,)),
            V((n_st, nb, 128), jnp.int32), pltpu.SMEM((n_st, nb, 128), jnp.int32),
            DMA((n_st,)), DMA((n_st,)), DMA,
            V((n_st, T, HW), BF), V((T, HW), BF), DMA((n_st - 1, n_tp)), DMA((n_st, n_tp)),
            V((2 * P_, PR, HW), BF), V((2 * P_, PR, HW), BF), V((P_, PR, HW), BF), V((P_, PR, HW), BF),
            DMA((2, R // 256)), DMA((2, R // 256)),
            V((T // SEQ_LEN, SEQ_LEN + 2 * pad, CL), F32), V((T, CL), F32), V((T, 128), F32),
            V((n_tp, 8, T), F32), DMA((n_tp,)), DMA((n_tp,)), V((T, CL), BF),
            V((n_st, T, HW), BF), V((n_st, n_tp, 8, T // n_tp), F32), V((n_st, T, HW), BF),
            V((n_st, n_tp, 8, T // n_tp), F32),
            DMA((n_st, n_tp)), DMA((n_st, n_tp)), DMA((n_st, n_tp)), DMA((n_st, n_tp)),
            V((T, D), BF), V((n_tp, T // n_tp, D), BF), V((n_tp, T // n_tp, D), BF),
            DMA((2, n_tp, SUB)), DMA((2, n_tp, SUB)),
        ],
        compiler_params=pltpu.CompilerParams(
            collective_id=0, has_side_effects=True, vmem_limit_bytes=60 * 1024 * 1024),
        name="layer",
    )(
        tokens, store.reshape(R, D), ids, mix_gain.reshape(1, D), glu_value, glu_gate, conv_taps,
        channel_gain.reshape(1, CL), mix_out, query_gain.reshape(1, D), passage_gain.reshape(1, D),
        query_proj, key_proj, value_proj, attn_out, blend_gain.reshape(1, D),
    )


def solution(mesh):
    in_specs = (
        P(("grp", "st"), None),
        P(("grp", "st"), None, None),
        P(("grp", "st"), None),
        P(),
        P(None, "tp"),
        P(None, "tp"),
        P(None, "tp"),
        P("tp"),
        P("tp", None),
        P(),
        P(),
        P(None, "tp"),
        P(None, "tp"),
        P(None, "tp"),
        P("tp", None),
        P(),
    )
    out_specs = P(("grp", "st", "tp"), None)
    def body(*args):
        even = args[11].shape[1] // HD % 2 == 0 and mesh.shape["st"] % 2 == 0
        even = even and args[2].shape[0] % mesh.shape["tp"] == 0 and mesh.shape["st"] <= 16
        return (fused_local if even else local)(*args)

    return jax.shard_map(body, mesh=mesh, in_specs=in_specs, out_specs=out_specs, check_vma=False)
```

```python
import functools

import jax
import jax.numpy as jnp
from jax import lax
from jax.sharding import PartitionSpec as P
from jax.experimental import pallas as pl
from jax.experimental.pallas import tpu as pltpu

CA = 1024
HD = 256
SEQ_LEN = 128


EPS = 1e-06


def rms_rows(row_data, gain_vec):
    floats = row_data.astype(jnp.float32)
    inv_scale = lax.rsqrt(jnp.mean(floats * floats, axis=-1, keepdims=True) + EPS)
    return (floats * inv_scale * gain_vec).astype(jnp.bfloat16)


def depthwise(gated_rows, conv_taps):
    span_width = conv_taps.shape[0]
    half_span = (span_width - 1) // 2
    seq_length = gated_rows.shape[1]
    padded = jnp.pad(
        gated_rows.astype(jnp.float32), ((0, 0), (half_span, span_width - 1 - half_span), (0, 0))
    )
    running = jnp.zeros(gated_rows.shape, jnp.float32)
    for tap_index in range(span_width):
        running = running + padded[:, tap_index : tap_index + seq_length] * conv_taps[
            tap_index
        ].astype(jnp.float32)
    return running


def passage_attention(queries, keys_values, head_count):
    groups, block_len, span_width = queries.shape
    head_dim = span_width // head_count
    row_count = keys_values.shape[1]
    query_heads = queries.reshape(groups, block_len, head_count, head_dim)
    key_heads = keys_values[:, :, :span_width].reshape(groups, row_count, head_count, head_dim)
    value_heads = keys_values[:, :, span_width:].reshape(groups, row_count, head_count, head_dim)
    scores = jnp.einsum(
        "gqhd,grhd->ghqr", query_heads, key_heads, preferred_element_type=jnp.float32
    ) * head_dim ** (-0.5)
    row_top = jnp.max(scores, axis=-1)
    exponent = jnp.exp(scores - row_top[..., None])
    row_sum = jnp.sum(exponent, axis=-1)
    weights = exponent.astype(jnp.bfloat16)
    outputs = jnp.einsum(
        "ghqr,grhd->gqhd", weights, value_heads, preferred_element_type=jnp.float32
    ).astype(jnp.bfloat16)
    return (outputs.reshape(groups, block_len, span_width), row_top, row_sum)


def combine(outs, tops, sums, head_count):
    batch_count, passage_count, block_len, span_width = outs.shape
    head_dim = span_width // head_count
    best_top = jnp.max(tops, axis=1, keepdims=True)
    weight = jnp.exp(tops - best_top)
    numerator = jnp.einsum(
        "bphq,bpqhd->bqhd",
        weight,
        outs.astype(jnp.float32).reshape(
            batch_count, passage_count, block_len, head_count, head_dim
        ),
    )
    denominator = jnp.sum(weight * sums, axis=1)
    result = numerator / jnp.transpose(denominator, (0, 2, 1))[..., None]
    return result.reshape(batch_count, block_len, span_width).astype(jnp.bfloat16)


def local(
    tokens,
    store,
    passage_ids,
    mix_gain,
    glu_value,
    glu_gate,
    conv_taps,
    channel_gain,
    mix_out,
    query_gain,
    passage_gain,
    query_proj,
    key_proj,
    value_proj,
    attn_out,
    blend_gain,
):
    owners = lax.axis_size("st")
    tok_rows = tokens.shape[0]
    model_width = tokens.shape[1]
    local_channels = glu_value.shape[1]
    head_width = query_proj.shape[1]
    local_heads = head_width // HD
    block_count = passage_ids.shape[0]
    per_block = passage_ids.shape[1]
    block_len = tok_rows // block_count
    requests = block_count * per_block
    capacity = 2 * requests // owners
    pass_local = store.shape[0]
    pass_rows = store.shape[1]
    flat_ids = passage_ids.reshape(requests)
    owner_of = flat_ids // pass_local
    local_of = flat_ids - owner_of * pass_local
    request_index = jnp.arange(requests)
    earlier = (owner_of[:, None] == owner_of[None, :]) & (
        request_index[None, :] < request_index[:, None]
    )
    ranking = jnp.sum(earlier.astype(jnp.int32), axis=1)
    slot_of = owner_of * capacity + ranking
    slot_ids = (
        jnp.zeros((owners * capacity,), jnp.int32)
        .at[slot_of]
        .set(local_of)
        .reshape(owners, capacity)
    )
    asked = lax.all_to_all(slot_ids, "st", split_axis=0, concat_axis=0, tiled=True)
    normed_store = rms_rows(store.reshape(pass_local * pass_rows, model_width), passage_gain)
    key_rows = jnp.dot(normed_store, key_proj, preferred_element_type=jnp.float32).astype(
        jnp.bfloat16
    )
    value_rows = jnp.dot(normed_store, value_proj, preferred_element_type=jnp.float32).astype(
        jnp.bfloat16
    )
    memory = jnp.concatenate([key_rows, value_rows], axis=1).reshape(
        pass_local, pass_rows, 2 * head_width
    )
    queries = jnp.dot(
        rms_rows(tokens, query_gain), query_proj, preferred_element_type=jnp.float32
    ).astype(jnp.bfloat16)
    query_blocks = queries.reshape(block_count, block_len, head_width)
    repeated = jnp.repeat(query_blocks, per_block, axis=0)
    served = memory[asked.reshape(owners * capacity)]
    slot_queries = (
        jnp.zeros((owners * capacity, block_len, head_width), jnp.bfloat16)
        .at[slot_of]
        .set(repeated)
    )
    visiting = lax.all_to_all(
        slot_queries.reshape(owners, capacity, block_len, head_width),
        "st",
        split_axis=0,
        concat_axis=0,
        tiled=True,
    )
    answer_out, answer_top, answer_sum = passage_attention(
        visiting.reshape(owners * capacity, block_len, head_width), served, local_heads
    )
    back_out = lax.all_to_all(
        answer_out.reshape(owners, capacity, block_len, head_width),
        "st",
        split_axis=0,
        concat_axis=0,
        tiled=True,
    )
    back_top, back_sum = (
        lax.all_to_all(
            answer_top.reshape(owners, capacity, local_heads, block_len),
            "st",
            split_axis=0,
            concat_axis=0,
            tiled=True,
        ),
        lax.all_to_all(
            answer_sum.reshape(owners, capacity, local_heads, block_len),
            "st",
            split_axis=0,
            concat_axis=0,
            tiled=True,
        ),
    )
    partial_out = back_out.reshape(owners * capacity, block_len, head_width)[slot_of]
    partial_top = back_top.reshape(owners * capacity, local_heads, block_len)[slot_of]
    partial_sum = back_sum.reshape(owners * capacity, local_heads, block_len)[slot_of]
    attended = combine(
        partial_out.reshape(block_count, per_block, block_len, head_width),
        partial_top.reshape(block_count, per_block, local_heads, block_len),
        partial_sum.reshape(block_count, per_block, local_heads, block_len),
        local_heads,
    ).reshape(tok_rows, head_width)
    mix_input = rms_rows(tokens, mix_gain)
    value_part = jnp.dot(mix_input, glu_value, preferred_element_type=jnp.float32)
    gate_part = jnp.dot(mix_input, glu_gate, preferred_element_type=jnp.float32)
    gated_rows = (value_part * jax.nn.sigmoid(gate_part)).astype(jnp.bfloat16)
    conv_rows = depthwise(gated_rows.reshape(-1, SEQ_LEN, local_channels), conv_taps).reshape(
        tok_rows, local_channels
    )
    channel_sum, channel_square = lax.psum(
        (jnp.sum(conv_rows, axis=1), jnp.sum(conv_rows * conv_rows, axis=1)), "tp"
    )
    row_mean = channel_sum / CA
    row_var = channel_square / CA - row_mean * row_mean
    activation = jax.nn.silu(
        (conv_rows - row_mean[:, None]) * lax.rsqrt(row_var + EPS)[:, None] * channel_gain
    ).astype(jnp.bfloat16)
    conv_term = jnp.dot(activation, mix_out, preferred_element_type=jnp.float32)
    attn_term = jnp.dot(attended, attn_out, preferred_element_type=jnp.float32)
    return lax.psum_scatter(
        (conv_term + blend_gain * attn_term).astype(jnp.bfloat16),
        "tp",
        scatter_dimension=0,
        tiled=True,
    )


BF = jnp.bfloat16
F32 = jnp.float32
NEG = -3e38


def mm(a, b):
    return jnp.dot(a, b, preferred_element_type=F32)


def wait_in(ref, sem):
    pltpu.make_async_copy(ref, ref, sem).wait()


def layer_kernel(
    n_st, n_tp, block_count, per_block, block_len, local_heads, seq_len, pass_rows,
    tokens_h, store_h, ids_v, mix_gain, gv_h, gg_h, taps, channel_gain, mo_h, query_gain,
    passage_gain, qw_h, kw_h, vw_h, ao_h, blend_gain,
    out_ref,
    tok, sto, gv, gg, mo, qw, kw, vw, ao, load_sem,
    ids_all, ids_s, ids_send, ids_recv, ids_sem,
    q_all, q_stage, q_send, q_recv,
    k_all, v_all, k_stage, v_stage, kv_send, kv_recv,
    gp, conv, scol, stat_all, stat_send, stat_recv, act,
    out_o, out_s, ret_o, ret_s, o_send, o_recv, s_send, s_recv,
    part, from_left, from_right, r_send, r_recv,
):
    st = lax.axis_index("st")
    tp = lax.axis_index("tp")
    core = lax.rem(st, 2)
    chip = st // 2
    n_chip = n_st // 2
    other = 1 - core
    T = tok.shape[0]
    R = sto.shape[0]
    HW = q_stage.shape[1]
    CL = act.shape[1]

    loads = []
    for n, (a, b) in enumerate(
        [(tokens_h, tok), (qw_h, qw), (store_h, sto), (kw_h, kw), (vw_h, vw), (gv_h, gv),
         (gg_h, gg), (mo_h, mo), (ao_h, ao)]
    ):
        c = pltpu.make_async_copy(a, b, load_sem.at[n])
        c.start()
        loads.append(c)

    barrier = pltpu.get_barrier_semaphore()
    for i in range(1, n_st):
        pl.semaphore_signal(barrier, inc=1, device_id={"st": lax.rem(st + i, n_st)},
                            device_id_type=pl.DeviceIdType.MESH)
    for i in range(1, n_tp):
        pl.semaphore_signal(barrier, inc=1, device_id={"tp": lax.rem(tp + i, n_tp)},
                            device_id_type=pl.DeviceIdType.MESH)

    def remote(src, dst, ssem, rsem, axis, to):
        return pltpu.make_async_remote_copy(
            src_ref=src, dst_ref=dst, send_sem=ssem, recv_sem=rsem, device_id={axis: to},
            device_id_type=pl.DeviceIdType.MESH)

    chunk_rows = T // n_tp
    table = [sorted(range(n_tp), key=lambda d: -abs(d - t)) for t in range(n_tp)]

    def chunk_at(k):
        d = jnp.int32(table[0][k])
        for t in range(1, n_tp):
            d = jnp.where(tp == t, table[t][k], d)
        return d

    chunks = [chunk_at(k) for k in range(n_tp)]

    def chunk_ds(d):
        return pl.ds(pl.multiple_of(d * chunk_rows, chunk_rows), chunk_rows)

    def peers():
        res = [(chip * 2 + other, True, 0)]
        for j in range(1, n_chip):
            c = lax.rem(chip + j, n_chip)
            res.append((c * 2 + core, False, 2 * j - 1))
            res.append((c * 2 + other, True, 2 * j))
        return res

    loads[0].wait()
    loads[1].wait()
    TC = 256
    mine = pl.ds(pl.multiple_of(core * HW, HW), HW)
    theirs = pl.ds(pl.multiple_of(other * HW, HW), HW)

    def tok_chunk(i, carry):
        rows = pl.ds(pl.multiple_of(i * TC, TC), TC)
        x = tok[rows, :].astype(F32)
        y = x * lax.rsqrt(jnp.mean(x * x, axis=-1, keepdims=True) + EPS)
        qr = (y * query_gain[...]).astype(BF)
        q_all[st, rows, :] = mm(qr, qw[:, mine]).astype(BF)
        q_stage[rows, :] = mm(qr, qw[:, theirs]).astype(BF)
        tok[rows, :] = (y * mix_gain[...]).astype(BF)
        return carry

    lax.fori_loop(0, T // TC, tok_chunk, 0)

    pl.semaphore_wait(barrier, n_st - 1 + n_tp - 1)
    for i in range(1, n_st):
        remote(ids_v, ids_all.at[st], ids_send.at[i], ids_recv.at[st], "st",
               lax.rem(st + i, n_st)).start()
    ids_own = pltpu.make_async_copy(ids_v, ids_all.at[st], ids_recv.at[st])
    ids_own.start()

    def q_copies(k):
        rows = chunk_ds(chunks[k])
        for to, stage, n in peers():
            src = q_stage.at[rows] if stage else q_all.at[st, rows]
            yield remote(src, q_all.at[st, rows], q_send.at[n, k], q_recv.at[st, k], "st", to)

    for k in range(n_tp):
        for c in q_copies(k):
            c.start()

    for n in range(2, 5):
        loads[n].wait()
    RC = 512
    n_rc = R // RC
    RP = RC // pass_rows
    pass_local = R // pass_rows
    partner = chip * 2 + other

    def store_chunk(i, carry):
        rows = pl.ds(pl.multiple_of(i * RC, RC), RC)
        x = sto[rows, :].astype(F32)
        n = (x * lax.rsqrt(jnp.mean(x * x, axis=-1, keepdims=True) + EPS) * passage_gain[...]).astype(BF)
        here, slots = pl.ds(i * RP, RP), pl.ds(core * pass_local + i * RP, RP)
        k_stage[here] = mm(n, kw[:, theirs]).astype(BF).reshape(RP, pass_rows, HW)
        v_stage[here] = mm(n, vw[:, theirs]).astype(BF).reshape(RP, pass_rows, HW)
        remote(k_stage.at[here], k_all.at[slots], kv_send.at[0, i], kv_recv.at[0, i], "st", partner).start()
        remote(v_stage.at[here], v_all.at[slots], kv_send.at[1, i], kv_recv.at[1, i], "st", partner).start()
        k_all[slots] = mm(n, kw[:, mine]).astype(BF).reshape(RP, pass_rows, HW)
        v_all[slots] = mm(n, vw[:, mine]).astype(BF).reshape(RP, pass_rows, HW)
        return carry

    lax.fori_loop(0, n_rc, store_chunk, 0)

    ids_own.wait()
    for i in range(1, n_st):
        r = lax.rem(st + i, n_st)
        remote(ids_v, ids_all.at[r], ids_send.at[i], ids_recv.at[r], "st", r).wait_recv()
    c = pltpu.make_async_copy(ids_all, ids_s, ids_sem)
    c.start()
    c.wait()

    def kv_wait(i, carry):
        here, slots = pl.ds(i * RP, RP), pl.ds(other * pass_local + i * RP, RP)
        remote(k_stage.at[here], k_all.at[slots], kv_send.at[0, i], kv_recv.at[0, i], "st", partner).wait()
        remote(v_stage.at[here], v_all.at[slots], kv_send.at[1, i], kv_recv.at[1, i], "st", partner).wait()
        return carry

    lax.fori_loop(0, n_rc, kv_wait, 0)

    heads = local_heads // 2
    HD_ = HW // heads
    per_chip = 2 * pass_local
    chunk_blocks = block_count // n_tp
    clane = lax.broadcasted_iota(jnp.int32, (chunk_rows, 128), 1)
    scale = HD_ ** (-0.5)

    def order(i):
        return lax.rem(chip + 1 + i // 2, n_chip) * 2 + lax.rem(core + 1 - i % 2, 2)

    def answer_copies(k, r):
        rows = chunk_ds(chunks[k])
        return (
            remote(out_o.at[r, rows], ret_o.at[st, rows], o_send.at[r, k], o_recv.at[st, k], "st", r),
            remote(out_s.at[r, k], ret_s.at[st, k], s_send.at[r, k], s_recv.at[st, k], "st", r),
        )

    def attend(k):
        d = chunks[k]
        rows = chunk_ds(d)

        def one(i, carry):
            r = order(i)

            @pl.when(i < n_st - 1)
            def _():
                remote(q_all.at[st, rows], q_all.at[r, rows], q_send.at[0, k], q_recv.at[r, k], "st", r).wait_recv()

            stats = jnp.zeros((chunk_rows, 128), F32)
            for h in range(heads):
                cols = slice(h * HD_, (h + 1) * HD_)
                tops, dens = [], []
                for u in range(chunk_blocks):
                    b = d * chunk_blocks + u
                    brow = pl.ds(pl.multiple_of(b * block_len, block_len), block_len)
                    q = q_all[r, brow, cols]
                    ks, vs, bias = [], [], []
                    for j in range(per_block):
                        p = ids_s[r, b, j] - chip * per_chip
                        spread_p = jnp.full((1, pass_rows), p, jnp.int32)
                        valid = jnp.logical_and(spread_p >= 0, spread_p < per_chip)
                        bias.append(jnp.where(valid, 0.0, NEG))
                        slot = jnp.clip(p, 0, per_chip - 1)
                        ks.append(k_all[slot][:, cols])
                        vs.append(v_all[slot][:, cols])
                    s = lax.dot_general(q, jnp.concatenate(ks, axis=0), (((1,), (1,)), ((), ())),
                                        preferred_element_type=F32)
                    s = s * scale + jnp.concatenate(bias, axis=1)
                    top = jnp.maximum(jnp.max(s, axis=1, keepdims=True), NEG / 2)
                    e = jnp.exp(s - top)
                    dens.append(jnp.sum(e, axis=1, keepdims=True))
                    tops.append(top)
                    out_o[r, brow, cols] = mm(e.astype(BF), jnp.concatenate(vs, axis=0)).astype(BF)
                stats = jnp.where(clane == 2 * h, jnp.concatenate(tops, axis=0), stats)
                stats = jnp.where(clane == 2 * h + 1, jnp.concatenate(dens, axis=0), stats)
            out_s[r, k] = jnp.transpose(stats)[:8]

            @pl.when(i < n_st - 1)
            def _():
                for c in answer_copies(k, r):
                    c.start()

            return carry

        lax.fori_loop(0, n_st, one, 0)

    attend(0)

    loads[5].wait()
    loads[6].wait()
    per_seq = seq_len
    pad = (gp.shape[1] - per_seq) // 2
    gp[:, :pad] = jnp.zeros((gp.shape[0], pad, CL), F32)
    gp[:, pad + per_seq:] = jnp.zeros((gp.shape[0], pad, CL), F32)

    def glu_chunk(i, carry):
        mr = tok[pl.ds(pl.multiple_of(i * TC, TC), TC), :]
        gated = (mm(mr, gv[...]) * jax.nn.sigmoid(mm(mr, gg[...]))).astype(BF).astype(F32)
        for u in range(TC // per_seq):
            gp[i * (TC // per_seq) + u, pad:pad + per_seq, :] = gated[u * per_seq:(u + 1) * per_seq]
        return carry

    lax.fori_loop(0, T // TC, glu_chunk, 0)
    tap_values = taps[...].astype(F32)
    n_tap = taps.shape[0]
    lead = pad - (n_tap - 1) // 2
    CC = 64
    per = per_seq // CC
    lane = lax.broadcasted_iota(jnp.int32, (CC, 128), 1)

    def conv_chunk(i, carry):
        seq = i // per
        base = pl.multiple_of(lax.rem(i, per) * CC, CC)
        win = gp[seq, pl.ds(base, CC + 2 * pad), :]
        acc = None
        for res in range(8):
            group = None
            for k in range(n_tap):
                if (lead + k) % 8 == res:
                    at = lead + k - res
                    term = win[at:at + CC + (8 if res else 0)] * tap_values[k:k + 1]
                    group = term if group is None else group + term
            if group is not None:
                group = group[res:res + CC]
                acc = group if acc is None else acc + group
        rows = pl.ds(pl.multiple_of(i * CC, CC), CC)
        conv[rows, :] = acc
        s = jnp.sum(acc, axis=1, keepdims=True)
        ss = jnp.sum(acc * acc, axis=1, keepdims=True)
        scol[rows, :] = jnp.where(lane == 0, s, jnp.where(lane == 1, ss, 0.0))
        return carry

    lax.fori_loop(0, T // CC, conv_chunk, 0)
    stat_all[tp] = jnp.transpose(scol[...])[:8]
    for i in range(1, n_tp):
        remote(stat_all.at[tp], stat_all.at[tp], stat_send.at[i], stat_recv.at[tp], "tp",
               lax.rem(tp + i, n_tp)).start()

    attend(1)

    total = stat_all[tp]
    for i in range(1, n_tp):
        r = lax.rem(tp + i, n_tp)
        remote(stat_all.at[tp], stat_all.at[r], stat_send.at[i], stat_recv.at[r], "tp", r).wait_recv()
        total = total + stat_all[r]
    ca = CL * n_tp
    mean = total / ca
    spread = jnp.transpose(jnp.concatenate([mean, jnp.zeros((120, T), F32)], axis=0))
    row_mean = spread[:, 0:1]
    inv = lax.rsqrt(spread[:, 1:2] - row_mean * row_mean + EPS)
    a = (conv[...] - row_mean) * inv * channel_gain[...]
    act[...] = (a / (1.0 + jnp.exp(-a))).astype(BF)
    loads[7].wait()
    loads[8].wait()

    SUB = 4
    SR = chunk_rows // SUB

    def hop(k, u, ahead, buf, way):
        d = chunks[k]
        prow = pl.ds(pl.multiple_of(d * chunk_rows + u * SR, SR), SR)
        brow = pl.ds(u * SR, SR)
        to = jnp.clip(tp + ahead, 0, n_tp - 1)
        return prow, brow, remote(part.at[prow], buf.at[d, brow], r_send.at[way, d, u],
                                  r_recv.at[way, d, u], "tp", to)

    ways = ((1, from_left, 0), (-1, from_right, 1))

    def goes(k, way):
        return tp < chunks[k] if way == 0 else tp > chunks[k]

    def at_end(way):
        return tp == 0 if way == 0 else tp == n_tp - 1

    def finish(k):
        rows = chunk_ds(chunks[k])
        for i in range(n_st - 1):
            r = order(i)
            remote(out_o.at[r, rows], ret_o.at[r, rows], o_send.at[r, k], o_recv.at[r, k], "st", r).wait_recv()
            remote(out_s.at[r, k], ret_s.at[r, k], s_send.at[r, k], s_recv.at[r, k], "st", r).wait_recv()
        ret_o[st, rows, :] = out_o[st, rows, :]
        ret_s[st, k] = out_s[st, k]
        stats = jnp.transpose(jnp.concatenate(
            [ret_s[c, k] for c in range(n_st)] + [jnp.zeros((128 - 8 * n_st, chunk_rows), F32)], axis=0))
        pieces = []
        for g in range(2):
            for h in range(heads):
                cols = slice(h * HD_, (h + 1) * HD_)
                at = [8 * (c * 2 + g) + 2 * h for c in range(n_chip)]
                best = functools.reduce(jnp.maximum, [stats[:, x:x + 1] for x in at])
                num, den = 0.0, 0.0
                for c in range(n_chip):
                    w = jnp.exp(stats[:, at[c]:at[c] + 1] - best)
                    num = num + w * ret_o[c * 2 + g, rows, cols].astype(F32)
                    den = den + w * stats[:, at[c] + 1:at[c] + 2]
                pieces.append((num / den).astype(BF))
        attended = jnp.concatenate(pieces, axis=1)
        act_rows = act[rows, :]
        NC = 512
        for i in range(part.shape[1] // NC):
            cols = slice(i * NC, (i + 1) * NC)
            value = mm(act_rows, mo[:, cols]) + blend_gain[:, cols] * mm(attended, ao[:, cols])
            part[rows, cols] = value.astype(BF)
        if k < n_tp - 1:
            for ahead, buf, way in ways:
                @pl.when(jnp.logical_and(goes(k, way), at_end(way)))
                def _(ahead=ahead, buf=buf, way=way):
                    for u in range(SUB):
                        hop(k, u, ahead, buf, way)[2].start()

    def forward(k, u):
        for ahead, buf, way in ways:
            @pl.when(jnp.logical_and(goes(k, way), jnp.logical_not(at_end(way))))
            def _(ahead=ahead, buf=buf, way=way):
                prow, brow, copy = hop(k, u, ahead, buf, way)
                copy.wait_recv()
                part[prow, :] = (part[prow, :].astype(F32) + buf[chunks[k], brow, :].astype(F32)).astype(BF)
                copy.start()

    forwarded = 0
    for k in range(n_tp):
        finish(k)
        if k + 2 < n_tp:
            attend(k + 2)
        elif k < n_tp - 1:
            for u in range(SUB):
                forward(k - 2, u)
            forwarded = k - 1
    for u in range(SUB):
        for k in range(forwarded, n_tp - 1):
            forward(k, u)

    for u in range(SUB):
        prow = pl.ds(pl.multiple_of(tp * chunk_rows + u * SR, SR), SR)
        brow = pl.ds(u * SR, SR)

        for ahead, buf, way in ways:
            @pl.when(jnp.logical_not(at_end(way)))
            def _(buf=buf, way=way, ahead=ahead):
                to = jnp.clip(tp - ahead, 0, n_tp - 1)
                remote(part.at[prow], buf.at[tp, brow], r_send.at[way, tp, u], r_recv.at[way, tp, u], "tp",
                       to).wait_recv()

            @pl.when(at_end(way))
            def _(buf=buf):
                buf[tp, brow, :] = jnp.zeros((SR, part.shape[1]), BF)

        out_ref[brow, :] = (
            part[prow, :].astype(F32) + from_left[tp, brow, :].astype(F32) + from_right[tp, brow, :].astype(F32)
        ).astype(BF)

    for i in range(1, n_st):
        r = lax.rem(st + i, n_st)
        remote(ids_v, ids_all.at[st], ids_send.at[i], ids_recv.at[st], "st", r).wait_send()
    for k in range(n_tp):
        for c in q_copies(k):
            c.wait_send()
        for i in range(n_st - 1):
            for c in answer_copies(k, order(i)):
                c.wait_send()
    for i in range(1, n_tp):
        remote(stat_all.at[tp], stat_all.at[tp], stat_send.at[i], stat_recv.at[tp], "tp",
               lax.rem(tp + i, n_tp)).wait_send()
    for k in range(n_tp - 1):
        for ahead, buf, way in ways:
            @pl.when(goes(k, way))
            def _(ahead=ahead, buf=buf, way=way):
                for u in range(SUB):
                    hop(k, u, ahead, buf, way)[2].wait_send()


def fused_local(
    tokens, store, passage_ids, mix_gain, glu_value, glu_gate, conv_taps, channel_gain, mix_out,
    query_gain, passage_gain, query_proj, key_proj, value_proj, attn_out, blend_gain,
):
    n_st = lax.axis_size("st")
    n_tp = lax.axis_size("tp")
    T, D = tokens.shape
    P_, PR, _ = store.shape
    R = P_ * PR
    W = query_proj.shape[1]
    HW = W // 2
    CL = glu_value.shape[1]
    nb, per_block = passage_ids.shape
    ids = jnp.pad(passage_ids, ((0, 0), (0, 128 - per_block)))
    pad = 8 * pl.cdiv((conv_taps.shape[0] - 1) // 2, 8)
    DMA = pltpu.SemaphoreType.DMA
    V = pltpu.VMEM
    SUB = 4
    kern = functools.partial(layer_kernel, n_st, n_tp, nb, per_block, T // nb, W // HD, SEQ_LEN, PR)
    hbm = pl.BlockSpec(memory_space=pl.ANY)
    vm = pl.BlockSpec(memory_space=pltpu.VMEM)
    return pl.pallas_call(
        kern,
        out_shape=jax.ShapeDtypeStruct((T // n_tp, D), BF),
        in_specs=[hbm, hbm, vm, vm, hbm, hbm, vm, vm, hbm, vm, vm, hbm, hbm, hbm, hbm, vm],
        out_specs=vm,
        scratch_shapes=[
            V((T, D), BF), V((R, D), BF), V((D, CL), BF), V((D, CL), BF), V((CL, D), BF),
            V((D, W), BF), V((D, W), BF), V((D, W), BF), V((W, D), BF), DMA((9,)),
            V((n_st, nb, 128), jnp.int32), pltpu.SMEM((n_st, nb, 128), jnp.int32),
            DMA((n_st,)), DMA((n_st,)), DMA,
            V((n_st, T, HW), BF), V((T, HW), BF), DMA((n_st - 1, n_tp)), DMA((n_st, n_tp)),
            V((2 * P_, PR, HW), BF), V((2 * P_, PR, HW), BF), V((P_, PR, HW), BF), V((P_, PR, HW), BF),
            DMA((2, R // 512)), DMA((2, R // 512)),
            V((T // SEQ_LEN, SEQ_LEN + 2 * pad, CL), F32), V((T, CL), F32), V((T, 128), F32),
            V((n_tp, 8, T), F32), DMA((n_tp,)), DMA((n_tp,)), V((T, CL), BF),
            V((n_st, T, HW), BF), V((n_st, n_tp, 8, T // n_tp), F32), V((n_st, T, HW), BF),
            V((n_st, n_tp, 8, T // n_tp), F32),
            DMA((n_st, n_tp)), DMA((n_st, n_tp)), DMA((n_st, n_tp)), DMA((n_st, n_tp)),
            V((T, D), BF), V((n_tp, T // n_tp, D), BF), V((n_tp, T // n_tp, D), BF),
            DMA((2, n_tp, SUB)), DMA((2, n_tp, SUB)),
        ],
        compiler_params=pltpu.CompilerParams(
            collective_id=0, has_side_effects=True, vmem_limit_bytes=60 * 1024 * 1024),
        name="layer",
    )(
        tokens, store.reshape(R, D), ids, mix_gain.reshape(1, D), glu_value, glu_gate, conv_taps,
        channel_gain.reshape(1, CL), mix_out, query_gain.reshape(1, D), passage_gain.reshape(1, D),
        query_proj, key_proj, value_proj, attn_out, blend_gain.reshape(1, D),
    )


def solution(mesh):
    in_specs = (
        P(("grp", "st"), None),
        P(("grp", "st"), None, None),
        P(("grp", "st"), None),
        P(),
        P(None, "tp"),
        P(None, "tp"),
        P(None, "tp"),
        P("tp"),
        P("tp", None),
        P(),
        P(),
        P(None, "tp"),
        P(None, "tp"),
        P(None, "tp"),
        P("tp", None),
        P(),
    )
    out_specs = P(("grp", "st", "tp"), None)
    def body(*args):
        even = args[11].shape[1] // HD % 2 == 0 and mesh.shape["st"] % 2 == 0
        even = even and args[2].shape[0] % mesh.shape["tp"] == 0 and mesh.shape["st"] <= 16
        return (fused_local if even else local)(*args)

    return jax.shard_map(body, mesh=mesh, in_specs=in_specs, out_specs=out_specs, check_vma=False)
```
